32 devices in a mesh: rep: 2 (over x), fs: 4 (over z), tp: 4 (over y, core).
Axes of the slice: x: 2, y: 2, z: 4, core: 2. Of those that a mesh axis runs over, the one named last changes fastest.
Arguments:
- tokens: bfloat16 [8192, 2048], P(('rep', 'fs', 'tp')), may hold values from -6 to 6
- cotangent: bfloat16 [8192, 2048], P(('rep', 'fs', 'tp')), may hold values from -6 to 6
- gate_weight: bfloat16 [2048, 3072], P('fs', 'tp'), may hold values from -0.125 to 0.125
- up_weight: bfloat16 [2048, 3072], P('fs', 'tp'), may hold values from -0.125 to 0.125
- down_weight: bfloat16 [3072, 2048], P('tp', 'fs'), may hold values from -0.109375 to 0.109375
Outputs:
- grad_tokens: bfloat16 [8192, 2048], P(('rep', 'fs', 'tp'))
- grad_gate: float32 [2048, 3072], P('fs', 'tp')
- grad_up: float32 [2048, 3072], P('fs', 'tp')
- grad_down: float32 [3072, 2048], P('tp', 'fs')
- gate_row_norms: float32 [2048], P('fs')
- up_row_norms: float32 [2048], P('fs')
- down_row_norms: float32 [3072], P('tp')
The draws below stay inside these ranges and needn't reach their ends.
All inputs are finite; a program needn't handle non-finite values.
Results may differ from the reference program's by a relative error of at most 0.014.
Values may be sent and summed in bfloat16 or wider, within the bound.
A program may use at most 128 MiB of HBM per device.

```python
import jax
import jax.numpy as jnp
from jax import lax

D = 2048
FF = 3072
TOKENS = 8192
N_TP = 4


def strengthened(entries, stream_key, source, target, blocks, factor):
    owner, partner = [(jnp.arange(entries.shape[dim]) // (entries.shape[dim] // blocks)).reshape([-1 if axis == dim else 1 for axis in range(entries.ndim)]) for dim in (source, target)]
    chosen = jax.random.permutation(stream_key, blocks)[partner]
    strong = (owner == chosen) | (owner == (partner + blocks // 2) % blocks)
    return jnp.where(strong, factor * entries, entries)


def shard_levels(rng, dims, pieces, low, largest):
    factor_of, own = 1.0, jax.random.fold_in(rng, 6)
    for dim, parts in pieces:
        draws = jnp.exp(jax.random.uniform(jax.random.fold_in(own, dim), (parts,), jnp.float32, low / len(pieces), largest / len(pieces)))
        factor_of = factor_of * jnp.repeat(draws, dims[dim] // parts).reshape([-1 if axis == dim else 1 for axis in range(len(dims))])
    return factor_of


def centred(stream_key, dims, scale, reach, cuts=(), held_as=jnp.bfloat16):
    loudness = shard_levels(stream_key, dims, cuts, -0.22, 0.18) if cuts else 1.0
    drawn = jax.random.normal(stream_key, dims, jnp.float32) * scale * loudness
    return jnp.minimum(jnp.maximum(drawn, -reach), reach).astype(held_as)


def gaussian_with(key, extent, spread, most, pieces, heavy, dtype=jnp.bfloat16):
    drawn = spread * jax.random.normal(key, extent, jnp.float32)
    if pieces:
        drawn = drawn * shard_levels(key, extent, pieces, -0.22, 0.18)
    return jnp.clip(strengthened(drawn, jax.random.fold_in(key, 3), *heavy), -most, most).astype(dtype)


def setup_inputs(seed: int = 0) -> dict:
    arg_keys = jax.random.split(jax.random.key(seed), 6)
    return {
        "tokens": centred(arg_keys[0], (TOKENS, D), 1.0, 6.0, ((0, 32),)),
        "cotangent": gaussian_with(arg_keys[1], (TOKENS, D), 1.0, 6.0, ((0, 32),), (0, 1, 32, 2.75)),
        "gate_weight": centred(arg_keys[2], (D, FF), D ** -0.5, 0.125, ((0, 4), (1, 4))),
        "up_weight": centred(arg_keys[3], (D, FF), D ** -0.5, 0.125, ((0, 4), (1, 4))),
        "down_weight": centred(arg_keys[4], (FF, D), FF ** -0.5, 0.109375, ((0, 4), (1, 4))),
    }


def reference(tokens, cotangent, gate_weight, up_weight, down_weight):
    gate = jnp.dot(tokens, gate_weight, preferred_element_type=jnp.float32)
    up = jnp.dot(tokens, up_weight, preferred_element_type=jnp.float32)
    sig = jax.nn.sigmoid(gate)
    act = gate * sig
    hidden = (act * up).astype(jnp.bfloat16)
    dhid = jnp.dot(cotangent, down_weight.T, preferred_element_type=jnp.float32)
    dgate = (dhid * up * sig * (1.0 + gate * (1.0 - sig))).astype(jnp.bfloat16)
    dup = (dhid * act).astype(jnp.bfloat16)
    grad_down = jnp.dot(hidden.T, cotangent, preferred_element_type=jnp.float32)
    grad_gate = jnp.dot(tokens.T, dgate, preferred_element_type=jnp.float32)
    grad_up = jnp.dot(tokens.T, dup, preferred_element_type=jnp.float32)
    block_width = FF // N_TP
    total = jnp.zeros(tokens.shape, jnp.float32)
    for block in range(N_TP):
        lower = block * block_width
        upper = lower + block_width
        partial_term = jnp.dot(dgate[:, lower:upper], gate_weight[:, lower:upper].T, preferred_element_type=jnp.float32)
        partial_term = partial_term + jnp.dot(dup[:, lower:upper], up_weight[:, lower:upper].T, preferred_element_type=jnp.float32)
        rounded = lax.optimization_barrier(partial_term.astype(jnp.bfloat16))
        total = total + rounded.astype(jnp.float32)
    grad_tokens = total.astype(jnp.bfloat16)
    gate_row_norms = jnp.sum(grad_gate * grad_gate, axis=1)
    up_row_norms = jnp.sum(grad_up * grad_up, axis=1)
    down_row_norms = jnp.sum(grad_down * grad_down, axis=1)
    return (grad_tokens, grad_gate, grad_up, grad_down, gate_row_norms, up_row_norms, down_row_norms)
```

```python
import functools

import jax
import jax.numpy as jnp
from jax import lax
from jax.experimental import pallas as pl
from jax.experimental.pallas import tpu as pltpu
from jax.sharding import PartitionSpec as P

F32, BF16 = jnp.float32, jnp.bfloat16
MESH = pl.DeviceIdType.MESH
DOWN, GATE, UP = 0, 1, 2


def contract_last(left, right):
    return lax.dot_general(
        left, right, (((1,), (1,)), ((), ())), preferred_element_type=F32
    )


def kernel(n, tps, sliced, tok_in, cot_in, wg_in, wu_in, wd_in,
           gt_out, gg_out, gu_out, gd_out, tn_out, fn_out,
           tok, cot, wg, wu, wd, act, coef, dh, hT, gT, uT, dg, du, own, rs, xs, xr,
           pc_s, pc_r, py_r, px_r, tnorm, fnorm,
           load_sem, ag_send, ag_recv, z_send, z_recv, rs_send, rs_recv, x_send, x_recv,
           pc_ss, pc_rs, py_ss, py_rs, px_ss, px_rs, tn_ss, tn_rs, fn_ss, fn_rs):
    ny = tps // 2
    r, f, t = lax.axis_index("rep"), lax.axis_index("fs"), lax.axis_index("tp")
    y, c = lax.div(t, 2), lax.rem(t, 2)
    R, D = tok_in.shape
    T, H = tok.shape[0], wg.shape[1]
    Dn = D // n
    tcore = t + 1 - 2 * c
    core_dev, x_dev = (r, f, tcore), (1 - r, f, t)
    ty = lambda dy: lax.rem(y + dy + ny, ny) * 2 + c
    y_dev = lambda dy: (r, f, ty(dy))
    right, left = (r, lax.rem(f + 1, n), t), (r, lax.rem(f + n - 1, n), t)

    def remote(src, dst, ss, rsem, dev):
        return pltpu.make_async_remote_copy(
            src_ref=src, dst_ref=dst, send_sem=ss, recv_sem=rsem,
            device_id=dev, device_id_type=MESH)

    def arrived(dst, sem):
        remote(dst, dst, sem, sem, core_dev).wait_recv()

    def rows(start, size):
        return pl.ds(pl.multiple_of(start, size), size)

    pending = []

    half = (lambda ref: ref.at[:, rows(r * H, H)]) if sliced else (lambda ref: ref)
    half_d = (lambda ref: ref.at[rows(r * H, H)]) if sliced else (lambda ref: ref)
    my_rows = rows((r * tps + t) * R, R)
    loads = [
        pltpu.make_async_copy(src, dst, load_sem.at[i]) for i, (src, dst) in enumerate([
            (tok_in, tok.at[my_rows]),
            (half(wg_in), wg.at[rows(f * Dn, Dn)]),
            (half(wu_in), wu.at[rows(f * Dn, Dn)]),
            (cot_in, cot.at[my_rows]),
            (half_d(wd_in), wd.at[:, rows(f * Dn, Dn)]),
        ])]
    for load in loads:
        load.start()

    barrier = pltpu.get_barrier_semaphore()
    for i in range(1, tps):
        pl.semaphore_signal(barrier, inc=1, device_id=(r, f, lax.rem(t + i, tps)), device_id_type=MESH)
    for i in range(1, n):
        pl.semaphore_signal(barrier, inc=1, device_id=(r, lax.rem(f + i, n), t), device_id_type=MESH)
    pl.semaphore_signal(barrier, inc=1, device_id=x_dev, device_id_type=MESH)
    pl.semaphore_wait(barrier, tps - 1 + n - 1 + 1)

    counts = [0, 0]
    bufs = (tok, cot)

    def part(a, slot, piece):
        if piece is None:
            return bufs[a].at[rows(slot * R, R)]
        return bufs[a].at[rows(slot * R + piece * (R // 2), R // 2)]

    def send_block(a, slot, piece, dev):
        view = part(a, slot, piece)
        copy = remote(view, view, ag_send.at[a, counts[a]], ag_recv.at[a, slot, piece or 0], dev)
        counts[a] += 1
        copy.start()
        pending.append(copy)

    def block_arrived(a, slot, piece):
        arrived(part(a, slot, piece), ag_recv.at[a, slot, piece or 0])

    slot_of = lambda rr, tt: rr * tps + tt

    def own_out(a):
        send_block(a, slot_of(r, t), None, x_dev)
        for dy in range(1, ny):
            send_block(a, slot_of(r, t), None, y_dev(dy))

    def own_core(a):
        send_block(a, slot_of(r, t), None, core_dev)

    def first_arrivals(a):
        slot = slot_of(1 - r, t)
        block_arrived(a, slot, None)
        for dy in range(1, ny):
            send_block(a, slot, 1, y_dev(dy))
        sent = [slot]
        for dy in range(1, ny):
            slot = slot_of(r, ty(-dy))
            block_arrived(a, slot, None)
            send_block(a, slot, 0, x_dev)
            sent.append(slot)
        return sent

    def to_core(a, slots):
        for slot in slots:
            send_block(a, slot, None, core_dev)

    def diagonal(a):
        for dy in range(1, ny):
            slot = slot_of(1 - r, ty(-dy))
            for piece in (0, 1):
                block_arrived(a, slot, piece)
                send_block(a, slot, piece, core_dev)

    def from_core(a):
        block_arrived(a, slot_of(r, tcore), None)
        block_arrived(a, slot_of(1 - r, tcore), None)
        for dy in range(1, ny):
            other = ty(dy) + 1 - 2 * c
            block_arrived(a, slot_of(r, other), None)
            for piece in (0, 1):
                block_arrived(a, slot_of(1 - r, other), piece)

    def weight(w, k):
        if w == DOWN:
            return wd.at[:, rows(k * Dn, Dn)]
        return (wg if w == GATE else wu).at[rows(k * Dn, Dn)]

    def weights_step(ws, s):
        for way, to, origin, has, sends in (
            (0, right, f - s, f - s >= 0, f + 1 < n),
            (1, left, f + s, f + s < n, f > 0),
        ):
            @pl.when(has)
            def _():
                for w in ws:
                    if s:
                        arrived(weight(w, origin), z_recv.at[w, origin])
                if s < n - 1:
                    @pl.when(sends)
                    def _():
                        for w in ws:
                            view = weight(w, origin)
                            remote(view, view, z_send.at[w, way, s], z_recv.at[w, origin], to).start()

    def weights_sent(ws):
        for s in range(n - 1):
            for way, to, origin, has, sends in (
                (0, right, f - s, f - s >= 0, f + 1 < n),
                (1, left, f + s, f + s < n, f > 0),
            ):
                @pl.when(jnp.logical_and(has, sends))
                def _():
                    for w in ws:
                        view = weight(w, origin)
                        remote(view, view, z_send.at[w, way, s], z_recv.at[w, origin], to).wait_send()

    for load in loads[:3]:
        load.wait()
    own_out(0)
    own_core(0)
    weights_step((GATE, UP), 0)
    for load in loads[3:]:
        load.wait()
    own_core(1)
    for s in range(1, n - 2):
        weights_step((GATE, UP), s)
    got = first_arrivals(0)
    own_out(1)
    to_core(0, got)
    for s in range(max(1, n - 2), n - 1):
        weights_step((GATE, UP), s)
    weights_step((DOWN,), 0)
    diagonal(0)
    from_core(0)
    weights_step((GATE, UP), n - 1)

    MB = min(512, T)
    EB = 128

    @pl.loop(0, T // MB)
    def _(i):
        blk = rows(i * MB, MB)
        act[blk] = jnp.dot(tok[blk], wg[...], preferred_element_type=F32)
        coef[blk] = jnp.dot(tok[blk], wu[...], preferred_element_type=F32)

    @pl.loop(0, T // EB)
    def _(i):
        blk = rows(i * EB, EB)
        gate, up = act[blk], coef[blk]
        sig = jax.nn.sigmoid(gate)
        a = gate * sig
        act[blk] = a
        coef[blk] = up * sig * (1.0 + gate * (1.0 - sig))
        hT[:, blk] = (a * up).astype(BF16).T

    got = first_arrivals(1)
    to_core(1, got)
    for s in range(1, n - 1):
        weights_step((DOWN,), s)
    diagonal(1)
    from_core(1)

    sources = {DOWN: (hT, cot), GATE: (gT, tok), UP: (uT, tok)}

    def own_part(w, d):
        lhs, rhs = sources[w]
        own[...] = jnp.dot(lhs[...], rhs[:, rows(d * Dn, Dn)], preferred_element_type=F32)

    def grads_out(w):
        @pl.loop(0, n - 1)
        def _(i):
            dist = n - 1 - i
            for to, d, has, more in (
                (right, f + dist, f + dist < n, f > 0),
                (left, f - dist, f - dist >= 0, f < n - 1),
            ):
                @pl.when(has)
                def _():
                    own_part(w, d)

                    @pl.when(more)
                    def _():
                        arrived(rs.at[w, d], rs_recv.at[w, d])
                        rs[w, d] = (own[...] + rs[w, d].astype(F32)).astype(BF16)

                    @pl.when(jnp.logical_not(more))
                    def _():
                        rs[w, d] = own[...].astype(BF16)

                    there = d if to is right else jnp.where(d == f - 1, n, d)
                    remote(rs.at[w, d], rs.at[w, there], rs_send.at[w, d], rs_recv.at[w, there], to).start()

    def grads_sent(w):
        @pl.loop(0, n)
        def _(d):
            @pl.when(d != f)
            def _():
                remote(rs.at[w, d], rs.at[w, d], rs_send.at[w, d], rs_recv.at[w, d], right).wait_send()

    def grads_final(w):
        own_part(w, f)

        @pl.when(f > 0)
        def _():
            arrived(rs.at[w, f], rs_recv.at[w, f])
            own[...] += rs[w, f].astype(F32)

        @pl.when(f < n - 1)
        def _():
            arrived(rs.at[w, n], rs_recv.at[w, n])
            own[...] += rs[w, n].astype(F32)

        xs[w] = own[...].astype(BF16)
        remote(xs.at[w], xr.at[w], x_send.at[w], x_recv.at[w], x_dev).start()

    grads_out(DOWN)
    weights_step((DOWN,), n - 1)

    @pl.loop(0, T // MB)
    def _(i):
        blk = rows(i * MB, MB)
        dh[blk] = contract_last(cot[blk], wd[...])

    @pl.loop(0, T // EB)
    def _(i):
        blk = rows(i * EB, EB)
        dhid = dh[blk]
        a = (dhid * coef[blk]).astype(BF16)
        b = (dhid * act[blk]).astype(BF16)
        dg[blk] = a
        du[blk] = b
        gT[:, blk] = a.T
        uT[:, blk] = b.T

    KB = min(512, D)

    def partial(slot, finish):
        blk = rows(slot * R, R)

        @pl.loop(0, D // KB)
        def _(k):
            cols = rows(k * KB, KB)
            finish(cols, contract_last(dg[blk], wg[cols]) + contract_last(du[blk], wu[cols]))

    for i in range(2 * ny):
        def put(cols, value):
            pc_s[i, :, cols] = value.astype(BF16)
        partial(slot_of(i // ny, (i % ny) * 2 + 1 - c), put)
        copy = remote(pc_s.at[i], pc_r.at[i], pc_ss.at[i], pc_rs.at[i], core_dev)
        copy.start()
        pending.append(copy)
    grads_out(GATE)

    for part_r in (1 - r, r):
        for dy in list(range(1, ny)) + [0]:
            yy = lax.rem(y + dy, ny)
            i = part_r * ny + yy
            arrived(pc_r.at[i], pc_rs.at[i])

            def put(cols, value):
                pc_r[i, :, cols] = (value + pc_r[i, :, cols].astype(F32)).astype(BF16)
            partial(slot_of(part_r, yy * 2 + c), put)
            if dy:
                copy = remote(pc_r.at[i], py_r.at[dy - 1, part_r], py_ss.at[dy - 1, part_r],
                              py_rs.at[dy - 1, part_r], y_dev(dy))
                copy.start()
                pending.append(copy)
    grads_out(UP)
    grads_final(DOWN)

    def add_y(part_r):
        i = part_r * ny + y
        for dy in range(1, ny):
            arrived(py_r.at[dy - 1, part_r], py_rs.at[dy - 1, part_r])

    add_y(1 - r)
    iother = (1 - r) * ny + y
    EC = 64

    @pl.loop(0, R // EC)
    def _(k):
        blk = rows(k * EC, EC)
        total = pc_r[iother, blk].astype(F32)
        for dy in range(1, ny):
            total += py_r[dy - 1, 1 - r, blk].astype(F32)
        pc_r[iother, blk] = total.astype(BF16)

    copy = remote(pc_r.at[iother], px_r, px_ss, px_rs, x_dev)
    copy.start()
    pending.append(copy)
    grads_final(GATE)
    grads_final(UP)

    def squares(value):
        return jnp.sum(value * value, axis=0, keepdims=True)

    tnorm[t] = jnp.zeros(tnorm.shape[1:], F32)
    fnorm[f] = jnp.zeros(fnorm.shape[1:], F32)

    def finish(w, buf, out, at):
        value = buf.astype(F32)
        turned = value.T
        if w == DOWN:
            out[at] = buf
            return squares(turned)
        out[at] = turned.astype(BF16)
        return squares(value)

    def exchange_norms(table, me, count, ss, rsem, dev):
        for i in range(1, count):
            copy = remote(table.at[me], table.at[me], ss.at[i - 1], rsem.at[me], dev(i))
            copy.start()
            pending.append(copy)

    arrived(xr.at[DOWN], x_recv.at[DOWN])
    fnorm[f, pl.ds(r, 1)] = finish(DOWN, xs[DOWN], gd_out, r)
    fnorm[f, pl.ds(1 - r, 1)] = finish(DOWN, xr[DOWN], gd_out, 1 - r)
    exchange_norms(fnorm, f, n, fn_ss, fn_rs, lambda i: (r, lax.rem(f + i, n), t))
    for row, (w, out) in enumerate(((GATE, gg_out), (UP, gu_out))):
        arrived(xr.at[w], x_recv.at[w])
        mine = finish(w, xs[w], out, r)
        theirs = finish(w, xr[w], out, 1 - r)
        tnorm[t, pl.ds(row, 1)] = mine + theirs
    exchange_norms(tnorm, t, tps, tn_ss, tn_rs, lambda i: (r, f, lax.rem(t + i, tps)))

    add_y(r)
    arrived(px_r, px_rs)
    imine = r * ny + y

    @pl.loop(0, R // EC)
    def _(k):
        blk = rows(k * EC, EC)
        total = pc_r[imine, blk].astype(F32) + px_r[blk].astype(F32)
        for dy in range(1, ny):
            total += py_r[dy - 1, r, blk].astype(F32)
        gt_out[blk] = total.astype(BF16)

    for i in range(1, n):
        k = lax.rem(f + i, n)
        arrived(fnorm.at[k], fn_rs.at[k])
    fn_out[...] = jnp.sum(fnorm[...], axis=0)
    for i in range(1, tps):
        k = lax.rem(t + i, tps)
        arrived(tnorm.at[k], tn_rs.at[k])
    tn_out[...] = jnp.sum(tnorm[...], axis=0)

    for copy in pending:
        copy.wait_send()
    weights_sent((GATE, UP, DOWN))
    for w in (DOWN, GATE, UP):
        grads_sent(w)
        remote(xs.at[w], xr.at[w], x_send.at[w], x_recv.at[w], x_dev).wait_send()


def local(tokens, cotangent, gate_weight, up_weight, down_weight):
    n, tps = lax.axis_size("fs"), lax.axis_size("tp")
    ny = tps // 2
    R, D = tokens.shape
    H = gate_weight.shape[1] // 2
    T, Dn = 2 * tps * R, D // n
    sliced = H % 128 == 0
    if not sliced:
        r = lax.axis_index("rep")
        gate_weight = lax.dynamic_slice_in_dim(gate_weight, r * H, H, 1)
        up_weight = lax.dynamic_slice_in_dim(up_weight, r * H, H, 1)
        down_weight = lax.dynamic_slice_in_dim(down_weight, r * H, H, 0)
    blocks = 2 * tps
    vmem = pltpu.VMEM
    dma = lambda *shape: pltpu.SemaphoreType.DMA(shape)
    shape = jax.ShapeDtypeStruct
    any_spec, vmem_spec = pl.BlockSpec(memory_space=pl.ANY), pl.BlockSpec(memory_space=vmem)
    flops = 2 * 8 * T * D * H
    gt, gg, gu, gd, tn, fn = pl.pallas_call(
        functools.partial(kernel, n, tps, sliced),
        out_shape=(
            shape((R, D), BF16), shape((2, Dn, H), BF16), shape((2, Dn, H), BF16),
            shape((2, H, Dn), BF16), shape((8, Dn), F32), shape((8, H), F32)),
        in_specs=[any_spec] * 5,
        out_specs=(vmem_spec,) * 6,
        scratch_shapes=[
            vmem((T, D), BF16), vmem((T, D), BF16),
            vmem((D, H), BF16), vmem((D, H), BF16), vmem((H, D), BF16),
            vmem((T, H), F32), vmem((T, H), F32), vmem((T, H), F32),
            vmem((H, T), BF16), vmem((H, T), BF16), vmem((H, T), BF16),
            vmem((T, H), BF16), vmem((T, H), BF16), vmem((H, Dn), F32),
            vmem((3, n + 1, H, Dn), BF16), vmem((3, H, Dn), BF16), vmem((3, H, Dn), BF16),
            vmem((2 * ny, R, D), BF16), vmem((2 * ny, R, D), BF16),
            vmem((max(ny - 1, 1), 2, R, D), BF16), vmem((R, D), BF16),
            vmem((tps, 8, Dn), F32), vmem((n, 8, H), F32),
            dma(5), dma(2, 4 * blocks), dma(2, blocks, 2), dma(3, 2, n), dma(3, n),
            dma(3, n), dma(3, n + 1), dma(3), dma(3),
            dma(2 * ny), dma(2 * ny), dma(max(ny - 1, 1), 2), dma(max(ny - 1, 1), 2),
            pltpu.SemaphoreType.DMA, pltpu.SemaphoreType.DMA, dma(tps), dma(tps), dma(n), dma(n),
        ],
        compiler_params=pltpu.CompilerParams(
            collective_id=0, has_side_effects=True, vmem_limit_bytes=67043328),
        cost_estimate=pl.CostEstimate(flops=flops, bytes_accessed=16 << 20, transcendentals=T * H),
    )(tokens, cotangent, gate_weight, up_weight, down_weight)
    wide = lambda part: jnp.concatenate([part[0], part[1]], axis=1).astype(F32)
    return (
        gt,
        wide(gg),
        wide(gu),
        gd.reshape(2 * H, Dn).astype(F32),
        tn[0],
        tn[1],
        jnp.concatenate([fn[0], fn[1]]),
    )


def solution(mesh):
    placed = (
        P(("rep", "fs", "tp"), None),
        P(("rep", "fs", "tp"), None),
        P("fs", "tp"),
        P("fs", "tp"),
        P("tp", "fs"),
    )
    return jax.shard_map(
        local,
        mesh=mesh,
        in_specs=placed,
        out_specs=(
            P(("rep", "fs", "tp"), None),
            P("fs", "tp"),
            P("fs", "tp"),
            P("tp", "fs"),
            P("fs"),
            P("fs"),
            P("tp"),
        ),
        check_vma=False,
    )
```

```python
import functools

import jax
import jax.numpy as jnp
from jax import lax
from jax.experimental import pallas as pl
from jax.experimental.pallas import tpu as pltpu
from jax.sharding import PartitionSpec as P

F32, BF16 = jnp.float32, jnp.bfloat16
MESH = pl.DeviceIdType.MESH
DOWN, GATE, UP = 0, 1, 2


def contract_last(left, right):
    return lax.dot_general(
        left, right, (((1,), (1,)), ((), ())), preferred_element_type=F32
    )


def kernel(n, tps, sliced, groups, tok_in, cot_in, wg_in, wu_in, wd_in,
           gt_out, gg_out, gu_out, gd_out, tn_out, fn_out,
           tok, cot, wg, wu, wd, act, coef, dh, hT, gT, uT, dg, du, own, rs, xs, xr,
           pc_s, pc_r, hx_r, hy_r, py_r, px_r, tnorm, fnorm,
           load_sem, ag_send, tok_recv, cot_recv, z_send, z_recv, rs_send, rs_recv,
           x_send, x_recv, pc_ss, pc_rs, hx_ss, hx_rs, hy_ss, hy_rs, py_ss, py_rs,
           px_ss, px_rs, tn_ss, tn_rs, fn_ss, fn_rs):
    ny = tps // 2
    r, f, t = lax.axis_index("rep"), lax.axis_index("fs"), lax.axis_index("tp")
    y, c = lax.div(t, 2), lax.rem(t, 2)
    R, D = tok_in.shape
    T, H = tok.shape[0], wg.shape[1]
    Dn, half_rows, chunk = D // n, R // 2, D // groups
    tcore = t + 1 - 2 * c
    core_dev, x_dev = (r, f, tcore), (1 - r, f, t)
    yat = lambda dy: lax.rem(y + dy + ny, ny)
    ty = lambda dy: yat(dy) * 2 + c
    y_dev = lambda dy: (r, f, ty(dy))
    right, left = (r, lax.rem(f + 1, n), t), (r, lax.rem(f + n - 1, n), t)
    others = range(1, ny)

    def remote(src, dst, ss, rsem, dev):
        return pltpu.make_async_remote_copy(
            src_ref=src, dst_ref=dst, send_sem=ss, recv_sem=rsem,
            device_id=dev, device_id_type=MESH)

    def arrived(dst, sem):
        remote(dst, dst, sem, sem, core_dev).wait_recv()

    def rows(start, size):
        return pl.ds(pl.multiple_of(start, size), size)

    pending = []

    def send(*args):
        copy = remote(*args)
        copy.start()
        pending.append(copy)

    half = (lambda ref: ref.at[:, rows(r * H, H)]) if sliced else (lambda ref: ref)
    half_d = (lambda ref: ref.at[rows(r * H, H)]) if sliced else (lambda ref: ref)
    my_rows = rows((r * tps + t) * R, R)
    loads = [
        pltpu.make_async_copy(src, dst, load_sem.at[i]) for i, (src, dst) in enumerate([
            (tok_in, tok.at[my_rows]),
            (half(wg_in), wg.at[rows(f * Dn, Dn)]),
            (half(wu_in), wu.at[rows(f * Dn, Dn)]),
            (cot_in, cot.at[my_rows]),
            (half_d(wd_in), wd.at[:, rows(f * Dn, Dn)]),
        ])]
    for load in loads:
        load.start()

    barrier = pltpu.get_barrier_semaphore()
    for i in range(1, tps):
        pl.semaphore_signal(barrier, inc=1, device_id=(r, f, lax.rem(t + i, tps)), device_id_type=MESH)
    for i in range(1, n):
        pl.semaphore_signal(barrier, inc=1, device_id=(r, lax.rem(f + i, n), t), device_id_type=MESH)
    pl.semaphore_signal(barrier, inc=1, device_id=x_dev, device_id_type=MESH)
    pl.semaphore_wait(barrier, tps - 1 + n - 1 + 1)

    sent = [0]

    def send_piece(view, sem, dev):
        send(view, view, ag_send.at[sent[0]], sem, dev)
        sent[0] += 1

    slot_of = lambda rr, tt: rr * tps + tt

    def tok_piece(slot, h):
        return tok.at[rows(slot * R + h * half_rows, half_rows)], tok_recv.at[slot, h]

    def cot_piece(slot, g, h):
        at = rows(slot * R, R) if h is None else rows(slot * R + h * half_rows, half_rows)
        return cot.at[at, rows(g * chunk, chunk)], cot_recv.at[slot, g, h or 0]

    mine, beside = slot_of(r, t), slot_of(1 - r, t)
    along = lambda dy: slot_of(r, ty(-dy))
    diagonal = lambda dy: slot_of(1 - r, ty(-dy))
    cored = lambda tt: tt + 1 - 2 * c

    def tok_out(to_x, to_y):
        send_piece(*tok_piece(mine, to_x), x_dev)
        for dy in others:
            send_piece(*tok_piece(mine, to_y), y_dev(dy))

    def tok_first():
        arrived(*tok_piece(beside, 1))
        for dy in others:
            send_piece(*tok_piece(beside, 1), y_dev(dy))
        for dy in others:
            arrived(*tok_piece(along(dy), 0))
            send_piece(*tok_piece(along(dy), 0), x_dev)

    def tok_first_core():
        send_piece(*tok_piece(beside, 1), core_dev)
        for dy in others:
            send_piece(*tok_piece(along(dy), 0), core_dev)

    def tok_second():
        for slot, h in [(beside, 0)] + [(along(dy), 1) for dy in others]:
            arrived(*tok_piece(slot, h))
            send_piece(*tok_piece(slot, h), core_dev)

    def tok_diagonal():
        for dy in others:
            for h in (0, 1):
                arrived(*tok_piece(diagonal(dy), h))
                send_piece(*tok_piece(diagonal(dy), h), core_dev)

    def tok_from_core():
        for dy in range(ny):
            for rr in (r, 1 - r):
                for h in (0, 1):
                    arrived(*tok_piece(slot_of(rr, cored(ty(dy))), h))

    def cot_out(g):
        send_piece(*cot_piece(mine, g, None), x_dev)
        for dy in others:
            send_piece(*cot_piece(mine, g, None), y_dev(dy))

    def cot_first(g):
        arrived(*cot_piece(beside, g, None))
        for dy in others:
            send_piece(*cot_piece(beside, g, 1), y_dev(dy))
        for dy in others:
            arrived(*cot_piece(along(dy), g, None))
            send_piece(*cot_piece(along(dy), g, 0), x_dev)

    def cot_first_core(g):
        for slot in [beside] + [along(dy) for dy in others]:
            send_piece(*cot_piece(slot, g, None), core_dev)

    def cot_diagonal(g):
        for dy in others:
            for h in (0, 1):
                arrived(*cot_piece(diagonal(dy), g, h))
                send_piece(*cot_piece(diagonal(dy), g, h), core_dev)

    def cot_from_core(g):
        arrived(*cot_piece(slot_of(r, tcore), g, None))
        arrived(*cot_piece(slot_of(1 - r, tcore), g, None))
        for dy in others:
            arrived(*cot_piece(slot_of(r, cored(ty(dy))), g, None))
            for h in (0, 1):
                arrived(*cot_piece(slot_of(1 - r, cored(ty(dy))), g, h))

    def weight(w, k):
        if w == DOWN:
            return wd.at[:, rows(k * Dn, Dn)]
        return (wg if w == GATE else wu).at[rows(k * Dn, Dn)]

    def ways(s):
        return ((0, right, f - s, f - s >= 0, f + 1 < n), (1, left, f + s, f + s < n, f > 0))

    def weights_step(w, s):
        for way, to, origin, has, sends in ways(s):
            @pl.when(has)
            def _():
                view = weight(w, origin)
                if s:
                    arrived(view, z_recv.at[w, origin])
                if s < n - 1:
                    @pl.when(sends)
                    def _():
                        remote(view, view, z_send.at[w, way, s], z_recv.at[w, origin], to).start()

    def weights_sent(w):
        for s in range(n - 1):
            for way, to, origin, has, sends in ways(s):
                @pl.when(jnp.logical_and(has, sends))
                def _():
                    view = weight(w, origin)
                    remote(view, view, z_send.at[w, way, s], z_recv.at[w, origin], to).wait_send()

    MB = min(512, T)
    EB = 128
    most = (n - 1) * Dn
    most_at = jnp.where(f == n - 1, Dn, 0)
    last_at = jnp.where(f == n - 1, 0, most)

    def gate_up_most(lo, hi):
        @pl.loop(lo, hi)
        def _(i):
            blk, cols = rows(i * MB, MB), pl.ds(pl.multiple_of(most_at, Dn), most)
            act[blk] = jnp.dot(tok[blk, cols], wg[cols], preferred_element_type=F32)
            coef[blk] = jnp.dot(tok[blk, cols], wu[cols], preferred_element_type=F32)

    def gate_up_last():
        @pl.loop(0, T // MB)
        def _(i):
            blk, cols = rows(i * MB, MB), rows(last_at, Dn)
            act[blk] += jnp.dot(tok[blk, cols], wg[cols], preferred_element_type=F32)
            coef[blk] += jnp.dot(tok[blk, cols], wu[cols], preferred_element_type=F32)

        @pl.loop(0, T // EB)
        def _(i):
            blk = rows(i * EB, EB)
            gate, up = act[blk], coef[blk]
            sig = jax.nn.sigmoid(gate)
            a = gate * sig
            act[blk] = a
            coef[blk] = up * sig * (1.0 + gate * (1.0 - sig))
            hT[:, blk] = (a * up).astype(BF16).T

    def hidden_grads():
        @pl.loop(0, T // MB)
        def _(i):
            blk = rows(i * MB, MB)
            dh[blk] = contract_last(cot[blk], wd[...])

        @pl.loop(0, T // EB)
        def _(i):
            blk = rows(i * EB, EB)
            dhid = dh[blk]
            a = (dhid * coef[blk]).astype(BF16)
            b = (dhid * act[blk]).astype(BF16)
            dg[blk] = a
            du[blk] = b
            gT[:, blk] = a.T
            uT[:, blk] = b.T

    sources = {DOWN: (hT, cot), GATE: (gT, tok), UP: (uT, tok)}

    def own_part(w, d):
        lhs, rhs = sources[w]
        own[...] = jnp.dot(lhs[...], rhs[:, rows(d * Dn, Dn)], preferred_element_type=F32)

    def grad_edge(w, d):
        @pl.when(jnp.where(f == 0, d > 0, jnp.logical_and(f == n - 1, d < n - 1)))
        def _():
            own_part(w, d)
            rs[w, d] = own[...].astype(BF16)
            there = jnp.where(jnp.logical_and(f > 0, d == f - 1), n, d)
            to = (r, jnp.where(f == 0, 1, n - 2), t)
            remote(rs.at[w, d], rs.at[w, there], rs_send.at[w, d], rs_recv.at[w, there], to).start()

    def grad_edge_group(w, g):
        per = n // groups

        @pl.loop(0, per)
        def _(i):
            grad_edge(w, g * per + i)

    def grad_edge_all(w):
        @pl.loop(0, n - 1)
        def _(i):
            grad_edge(w, jnp.where(f == 0, n - 1 - i, i))

    def grad_through(w, first, last):
        @pl.loop(0, first - last + 1)
        def _(i):
            dist = first - i
            for to, d, has in (
                (right, f + dist, jnp.logical_and(f + dist < n, f > 0)),
                (left, f - dist, jnp.logical_and(f - dist >= 0, f < n - 1)),
            ):
                @pl.when(has)
                def _():
                    own_part(w, d)
                    arrived(rs.at[w, d], rs_recv.at[w, d])
                    rs[w, d] = (own[...] + rs[w, d].astype(F32)).astype(BF16)
                    there = d if to is right else jnp.where(d == f - 1, n, d)
                    remote(rs.at[w, d], rs.at[w, there], rs_send.at[w, d], rs_recv.at[w, there], to).start()

    def grads_sent(w):
        @pl.loop(0, n)
        def _(d):
            @pl.when(d != f)
            def _():
                remote(rs.at[w, d], rs.at[w, d], rs_send.at[w, d], rs_recv.at[w, d], right).wait_send()

    def grad_final(w):
        own_part(w, f)

        @pl.when(f > 0)
        def _():
            arrived(rs.at[w, f], rs_recv.at[w, f])
            own[...] += rs[w, f].astype(F32)

        @pl.when(f < n - 1)
        def _():
            arrived(rs.at[w, n], rs_recv.at[w, n])
            own[...] += rs[w, n].astype(F32)

        xs[w] = own[...].astype(BF16)
        remote(xs.at[w], xr.at[w], x_send.at[w], x_recv.at[w], x_dev).start()

    KB = min(512, D)

    def partial(slot, finish):
        blk = rows(slot * R, R)

        @pl.loop(0, D // KB)
        def _(k):
            cols = rows(k * KB, KB)
            finish(cols, contract_last(dg[blk], wg[cols]) + contract_last(du[blk], wu[cols]))

    at_of = lambda rr, yy: rr * ny + yy

    def partial_for_core(rr, dy):
        i = at_of(rr, yat(dy))

        def put(cols, value):
            pc_s[i, :, cols] = value.astype(BF16)
        partial(slot_of(rr, cored(ty(dy))), put)
        send(pc_s.at[i], pc_r.at[i], pc_ss.at[i], pc_rs.at[i], core_dev)

    def partial_own(rr, dy):
        i = at_of(rr, yat(dy))
        arrived(pc_r.at[i], pc_rs.at[i])

        def put(cols, value):
            pc_r[i, :, cols] = (value + pc_r[i, :, cols].astype(F32)).astype(BF16)
        partial(slot_of(rr, ty(dy)), put)

    top, bottom = pl.ds(0, half_rows), pl.ds(half_rows, half_rows)

    def halves_out():
        for dy in others:
            i = at_of(1 - r, yat(dy))
            k = dy - 1
            send(pc_r.at[i, top], hx_r.at[k], hx_ss.at[k], hx_rs.at[k], x_dev)
            send(pc_r.at[i, bottom], hy_r.at[k], hy_ss.at[k], hy_rs.at[k], y_dev(dy))

    EC = 64

    def add_rows(i, base, terms):
        @pl.loop(0, half_rows // EC)
        def _(k):
            at = pl.ds(pl.multiple_of(base + k * EC, EC), EC)
            total = pc_r[i, at].astype(F32)
            for term in terms:
                total += term[pl.ds(pl.multiple_of(k * EC, EC), EC)].astype(F32)
            pc_r[i, at] = total.astype(BF16)

    def blocks_out():
        for dy in others:
            i = at_of(r, yat(dy))
            arrived(hx_r.at[dy - 1], hx_rs.at[dy - 1])
            add_rows(i, 0, [hx_r.at[dy - 1]])
            send(pc_r.at[i], py_r.at[dy - 1], py_ss.at[dy - 1], py_rs.at[dy - 1], y_dev(dy))
        i = at_of(1 - r, y)
        for dy in others:
            arrived(hy_r.at[dy - 1], hy_rs.at[dy - 1])
        add_rows(i, half_rows, [hy_r.at[dy - 1] for dy in others])
        send(pc_r.at[i], px_r, px_ss, px_rs, x_dev)

    def tokens_final():
        i = at_of(r, y)
        for dy in others:
            arrived(py_r.at[dy - 1], py_rs.at[dy - 1])
        arrived(px_r, px_rs)

        @pl.loop(0, R // EC)
        def _(k):
            at = rows(k * EC, EC)
            total = pc_r[i, at].astype(F32) + px_r[at].astype(F32)
            for dy in others:
                total += py_r[dy - 1, at].astype(F32)
            gt_out[at] = total.astype(BF16)

    def squares(value):
        return jnp.sum(value * value, axis=0, keepdims=True)

    def finish(w, buf, out, at):
        value = buf.astype(F32)
        turned = value.T
        if w == DOWN:
            out[at] = buf
            return squares(turned)
        if sliced:
            out[:, rows(at * H, H)] = turned.astype(BF16)
        else:
            out[at] = turned.astype(BF16)
        return squares(value)

    def finish_wide(w, row, out):
        arrived(xr.at[w], x_recv.at[w])
        tnorm[t, pl.ds(row, 1)] = finish(w, xs[w], out, r) + finish(w, xr[w], out, 1 - r)

    def finish_down():
        arrived(xr.at[DOWN], x_recv.at[DOWN])
        fnorm[f, pl.ds(r, 1)] = finish(DOWN, xs[DOWN], gd_out, r)
        fnorm[f, pl.ds(1 - r, 1)] = finish(DOWN, xr[DOWN], gd_out, 1 - r)

    def norms_out(table, me, count, ss, rsem, dev):
        for i in range(1, count):
            send(table.at[me], table.at[me], ss.at[i - 1], rsem.at[me], dev(i))

    def norms_in(table, me, count, rsem, out):
        for i in range(1, count):
            k = lax.rem(me + i, count)
            arrived(table.at[k], rsem.at[k])
        out[...] = jnp.sum(table[...], axis=0)

    order = []
    for g in range((groups + 1) // 2):
        order += [groups - 1 - g] + ([g] if g < groups - 1 - g else [])

    for load in loads[:3]:
        load.wait()
    tok_out(1, 0)
    weights_step(GATE, 0)
    weights_step(UP, 0)
    tok_out(0, 1)
    for h in (0, 1):
        send_piece(*tok_piece(mine, h), core_dev)
    for load in loads[3:]:
        load.wait()
    for g in order:
        send_piece(*cot_piece(mine, g, None), core_dev)
    tnorm[t] = jnp.zeros(tnorm.shape[1:], F32)
    fnorm[f] = jnp.zeros(fnorm.shape[1:], F32)
    if n > 2:
        weights_step(GATE, 1)
    tok_first()
    cot_out(order[0])
    tok_first_core()
    if n > 2:
        weights_step(UP, 1)
    tok_second()
    if groups > 1:
        cot_out(order[1])
    for s in range(2, n - 1):
        weights_step(GATE, s)
        weights_step(UP, s)
    weights_step(DOWN, 0)
    tok_diagonal()
    tok_from_core()
    steps = T // MB
    gate_up_most(0, steps // 2)

    def cot_next(k):
        cot_first(order[k])
        if k + 2 < groups:
            cot_out(order[k + 2])
        cot_first_core(order[k])

    cot_next(0)
    gate_up_most(steps // 2, steps)
    if groups > 1:
        cot_next(1)
    weights_step(GATE, n - 1)
    weights_step(UP, n - 1)
    cot_diagonal(order[0])
    gate_up_last()
    if groups > 2:
        cot_next(2)
    cot_from_core(order[0])
    grad_edge_group(DOWN, order[0])
    down_steps = list(range(1, n - 1))
    for s in down_steps[:1]:
        weights_step(DOWN, s)
    for k in range(1, groups):
        cot_diagonal(order[k])
        if k + 2 < groups:
            cot_next(k + 2)
        cot_from_core(order[k])
        grad_edge_group(DOWN, order[k])
        for s in down_steps[k:k + 1]:
            weights_step(DOWN, s)
    for s in down_steps[groups:]:
        weights_step(DOWN, s)
    if n > 2:
        grad_through(DOWN, n - 2, 2)
    weights_step(DOWN, n - 1)
    hidden_grads()
    grad_edge_all(GATE)
    if n > 2:
        grad_through(DOWN, 1, 1)
    pieces = ([(1 - r, dy) for dy in others] + [(r, dy) for dy in others] + [(1 - r, 0), (r, 0)])
    for rr, dy in pieces:
        partial_for_core(rr, dy)
    for rr, dy in pieces[:len(others)]:
        partial_own(rr, dy)
    halves_out()
    for rr, dy in pieces[len(others):]:
        partial_own(rr, dy)
    if n > 2:
        grad_through(GATE, n - 2, 2)
    grad_final(DOWN)
    grad_edge_all(UP)
    blocks_out()
    if n > 2:
        grad_through(GATE, 1, 1)
    finish_down()
    norms_out(fnorm, f, n, fn_ss, fn_rs, lambda i: (r, lax.rem(f + i, n), t))
    if n > 2:
        grad_through(UP, n - 2, 2)
    grad_final(GATE)
    if n > 2:
        grad_through(UP, 1, 1)
    tokens_final()
    finish_wide(GATE, 0, gg_out)
    norms_in(fnorm, f, n, fn_rs, fn_out)
    grad_final(UP)
    finish_wide(UP, 1, gu_out)
    norms_out(tnorm, t, tps, tn_ss, tn_rs, lambda i: (r, f, lax.rem(t + i, tps)))
    norms_in(tnorm, t, tps, tn_rs, tn_out)

    for copy in pending:
        copy.wait_send()
    for w in (DOWN, GATE, UP):
        weights_sent(w)
        grads_sent(w)
        remote(xs.at[w], xr.at[w], x_send.at[w], x_recv.at[w], x_dev).wait_send()


def local(tokens, cotangent, gate_weight, up_weight, down_weight):
    n, tps = lax.axis_size("fs"), lax.axis_size("tp")
    ny = tps // 2
    R, D = tokens.shape
    H = gate_weight.shape[1] // 2
    T, Dn = 2 * tps * R, D // n
    sliced = H % 128 == 0
    if not sliced:
        r = lax.axis_index("rep")
        gate_weight = lax.dynamic_slice_in_dim(gate_weight, r * H, H, 1)
        up_weight = lax.dynamic_slice_in_dim(up_weight, r * H, H, 1)
        down_weight = lax.dynamic_slice_in_dim(down_weight, r * H, H, 0)
    blocks = 2 * tps
    groups = min(n, 4)
    wide_shape = (Dn, 2 * H) if sliced else (2, Dn, H)
    more = max(ny - 1, 1)
    vmem = pltpu.VMEM
    dma = lambda *shape: pltpu.SemaphoreType.DMA(shape)
    shape = jax.ShapeDtypeStruct
    any_spec, vmem_spec = pl.BlockSpec(memory_space=pl.ANY), pl.BlockSpec(memory_space=vmem)
    flops = 2 * 8 * T * D * H
    gt, gg, gu, gd, tn, fn = pl.pallas_call(
        functools.partial(kernel, n, tps, sliced, groups),
        out_shape=(
            shape((R, D), BF16), shape(wide_shape, BF16), shape(wide_shape, BF16),
            shape((2, H, Dn), BF16), shape((8, Dn), F32), shape((8, H), F32)),
        in_specs=[any_spec] * 5,
        out_specs=(vmem_spec,) * 6,
        scratch_shapes=[
            vmem((T, D), BF16), vmem((T, D), BF16),
            vmem((D, H), BF16), vmem((D, H), BF16), vmem((H, D), BF16),
            vmem((T, H), F32), vmem((T, H), F32), vmem((T, H), F32),
            vmem((H, T), BF16), vmem((H, T), BF16), vmem((H, T), BF16),
            vmem((T, H), BF16), vmem((T, H), BF16), vmem((H, Dn), F32),
            vmem((3, n + 1, H, Dn), BF16), vmem((3, H, Dn), BF16), vmem((3, H, Dn), BF16),
            vmem((2 * ny, R, D), BF16), vmem((2 * ny, R, D), BF16),
            vmem((more, R // 2, D), BF16), vmem((more, R // 2, D), BF16),
            vmem((more, R, D), BF16), vmem((R, D), BF16),
            vmem((tps, 8, Dn), F32), vmem((n, 8, H), F32),
            dma(5), dma(12 * ny * (groups + 1)), dma(blocks, 2), dma(blocks, groups, 2),
            dma(3, 2, n), dma(3, n), dma(3, n), dma(3, n + 1), dma(3), dma(3),
            dma(2 * ny), dma(2 * ny), dma(more), dma(more), dma(more), dma(more),
            dma(more), dma(more), pltpu.SemaphoreType.DMA, pltpu.SemaphoreType.DMA,
            dma(tps), dma(tps), dma(n), dma(n),
        ],
        compiler_params=pltpu.CompilerParams(
            collective_id=0, has_side_effects=True, vmem_limit_bytes=67043328),
        cost_estimate=pl.CostEstimate(flops=flops, bytes_accessed=16 << 20, transcendentals=T * H),
    )(tokens, cotangent, gate_weight, up_weight, down_weight)
    def wide(part):
        if not sliced:
            part = jnp.concatenate([part[0], part[1]], axis=1)
        return part.astype(F32)
    return (
        gt,
        wide(gg),
        wide(gu),
        gd.reshape(2 * H, Dn).astype(F32),
        tn[0],
        tn[1],
        jnp.concatenate([fn[0], fn[1]]),
    )


def solution(mesh):
    placed = (
        P(("rep", "fs", "tp"), None),
        P(("rep", "fs", "tp"), None),
        P("fs", "tp"),
        P("fs", "tp"),
        P("tp", "fs"),
    )
    return jax.shard_map(
        local,
        mesh=mesh,
        in_specs=placed,
        out_specs=(
            P(("rep", "fs", "tp"), None),
            P("fs", "tp"),
            P("fs", "tp"),
            P("tp", "fs"),
            P("fs"),
            P("fs"),
            P("tp"),
        ),
        check_vma=False,
    )
```

```python
import functools

import jax
import jax.numpy as jnp
from jax import lax
from jax.experimental import pallas as pl
from jax.experimental.pallas import tpu as pltpu
from jax.sharding import PartitionSpec as P

F32, BF16 = jnp.float32, jnp.bfloat16
MESH = pl.DeviceIdType.MESH
DOWN, GATE, UP = 0, 1, 2


def contract_last(left, right):
    return lax.dot_general(
        left, right, (((1,), (1,)), ((), ())), preferred_element_type=F32
    )


def kernel(n, tps, sliced, groups, cuts, tok_in, cot_in, wg_in, wu_in, wd_in,
           gt_out, gg_out, gu_out, gd_out, tn_out, fn_out,
           tok, cot, wg, wu, wd, act, coef, dh, hT, gT, uT, dg, du, own, rs, xs, xr,
           pc_s, pc_r, py_r, px_r, turned, tnorm, fnorm, t_sum, f_sum,
           load_sem, ag_send, tok_recv, cot_recv, z_send, z_recv, rs_send, rs_recv,
           x_send, x_recv, pc_ss, pc_rs, py_ss, py_rs, px_ss, px_rs,
           tn_ss, tn_rs, fn_ss, fn_rs, out_sem):
    ny = tps // 2
    r, f, t = lax.axis_index("rep"), lax.axis_index("fs"), lax.axis_index("tp")
    y, c = lax.div(t, 2), lax.rem(t, 2)
    R, D = tok_in.shape
    T, H = tok.shape[0], wg.shape[1]
    Dn, half_rows, chunk = D // n, R // 2, D // groups
    tcore = t + 1 - 2 * c
    core_dev, x_dev = (r, f, tcore), (1 - r, f, t)
    yat = lambda dy: lax.rem(y + dy + ny, ny)
    ty = lambda dy: yat(dy) * 2 + c
    y_dev = lambda dy: (r, f, ty(dy))
    right, left = (r, lax.rem(f + 1, n), t), (r, lax.rem(f + n - 1, n), t)
    others = range(1, ny)

    def remote(src, dst, ss, rsem, dev):
        return pltpu.make_async_remote_copy(
            src_ref=src, dst_ref=dst, send_sem=ss, recv_sem=rsem,
            device_id=dev, device_id_type=MESH)

    def arrived(dst, sem):
        remote(dst, dst, sem, sem, core_dev).wait_recv()

    def rows(start, size):
        return pl.ds(pl.multiple_of(start, size), size)

    pending = []

    def send(*args):
        copy = remote(*args)
        copy.start()
        pending.append(copy)

    half = (lambda ref: ref.at[:, rows(r * H, H)]) if sliced else (lambda ref: ref)
    half_d = (lambda ref: ref.at[rows(r * H, H)]) if sliced else (lambda ref: ref)
    my_rows = rows((r * tps + t) * R, R)
    loads = [
        pltpu.make_async_copy(src, dst, load_sem.at[i]) for i, (src, dst) in enumerate([
            (tok_in, tok.at[my_rows]),
            (half(wg_in), wg.at[rows(f * Dn, Dn)]),
            (half(wu_in), wu.at[rows(f * Dn, Dn)]),
            (cot_in, cot.at[my_rows]),
            (half_d(wd_in), wd.at[:, rows(f * Dn, Dn)]),
        ])]
    for load in loads:
        load.start()

    barrier = pltpu.get_barrier_semaphore()
    for i in range(1, tps):
        pl.semaphore_signal(barrier, inc=1, device_id=(r, f, lax.rem(t + i, tps)), device_id_type=MESH)
    for i in range(1, n):
        pl.semaphore_signal(barrier, inc=1, device_id=(r, lax.rem(f + i, n), t), device_id_type=MESH)
    for i in range(tps):
        pl.semaphore_signal(barrier, inc=1, device_id=(1 - r, f, lax.rem(t + i, tps)), device_id_type=MESH)
    pl.semaphore_wait(barrier, tps - 1 + n - 1 + tps)

    sent = [0]

    def send_piece(view, sem, dev):
        send(view, view, ag_send.at[sent[0]], sem, dev)
        sent[0] += 1

    slot_of = lambda rr, tt: rr * tps + tt

    def tok_piece(slot, h):
        return tok.at[rows(slot * R + h * half_rows, half_rows)], tok_recv.at[slot, h]

    def cot_piece(slot, g, h):
        at = rows(slot * R, R) if h is None else rows(slot * R + h * half_rows, half_rows)
        return cot.at[at, rows(g * chunk, chunk)], cot_recv.at[slot, g, h or 0]

    mine, beside = slot_of(r, t), slot_of(1 - r, t)
    along = lambda dy: slot_of(r, ty(-dy))
    diagonal = lambda dy: slot_of(1 - r, ty(-dy))
    cored = lambda tt: tt + 1 - 2 * c

    def tok_out(to_x, to_y):
        send_piece(*tok_piece(mine, to_x), x_dev)
        for dy in others:
            send_piece(*tok_piece(mine, to_y), y_dev(dy))

    def tok_first():
        arrived(*tok_piece(beside, 1))
        for dy in others:
            send_piece(*tok_piece(beside, 1), y_dev(dy))
        for dy in others:
            arrived(*tok_piece(along(dy), 0))
            send_piece(*tok_piece(along(dy), 0), x_dev)

    def tok_first_core():
        send_piece(*tok_piece(beside, 1), core_dev)
        for dy in others:
            send_piece(*tok_piece(along(dy), 0), core_dev)

    def tok_second():
        for slot, h in [(beside, 0)] + [(along(dy), 1) for dy in others]:
            arrived(*tok_piece(slot, h))
            send_piece(*tok_piece(slot, h), core_dev)

    def tok_diagonal():
        for dy in others:
            for h in (0, 1):
                arrived(*tok_piece(diagonal(dy), h))
                send_piece(*tok_piece(diagonal(dy), h), core_dev)

    def tok_from_core():
        for dy in range(ny):
            for rr in (r, 1 - r):
                for h in (0, 1):
                    arrived(*tok_piece(slot_of(rr, cored(ty(dy))), h))

    def cot_out(g):
        send_piece(*cot_piece(mine, g, None), x_dev)
        for dy in others:
            send_piece(*cot_piece(mine, g, None), y_dev(dy))

    def cot_first(g):
        arrived(*cot_piece(beside, g, None))
        for dy in others:
            send_piece(*cot_piece(beside, g, 1), y_dev(dy))
        for dy in others:
            arrived(*cot_piece(along(dy), g, None))
            send_piece(*cot_piece(along(dy), g, 0), x_dev)

    def cot_first_core(g):
        for slot in [beside] + [along(dy) for dy in others]:
            send_piece(*cot_piece(slot, g, None), core_dev)

    def cot_diagonal(g):
        for dy in others:
            for h in (0, 1):
                arrived(*cot_piece(diagonal(dy), g, h))
                send_piece(*cot_piece(diagonal(dy), g, h), core_dev)

    def cot_from_core(g):
        arrived(*cot_piece(slot_of(r, tcore), g, None))
        arrived(*cot_piece(slot_of(1 - r, tcore), g, None))
        for dy in others:
            arrived(*cot_piece(slot_of(r, cored(ty(dy))), g, None))
            for h in (0, 1):
                arrived(*cot_piece(slot_of(1 - r, cored(ty(dy))), g, h))

    def weight(w, k):
        if w == DOWN:
            return wd.at[:, rows(k * Dn, Dn)]
        return (wg if w == GATE else wu).at[rows(k * Dn, Dn)]

    def ways(s):
        return ((0, right, f - s, f - s >= 0, f + 1 < n), (1, left, f + s, f + s < n, f > 0))

    def weights_step(w, s):
        for way, to, origin, has, sends in ways(s):
            @pl.when(has)
            def _():
                view = weight(w, origin)
                if s:
                    arrived(view, z_recv.at[w, origin])
                if s < n - 1:
                    @pl.when(sends)
                    def _():
                        remote(view, view, z_send.at[w, way, s], z_recv.at[w, origin], to).start()

    def weights_sent(w):
        for s in range(n - 1):
            for way, to, origin, has, sends in ways(s):
                @pl.when(jnp.logical_and(has, sends))
                def _():
                    view = weight(w, origin)
                    remote(view, view, z_send.at[w, way, s], z_recv.at[w, origin], to).wait_send()

    MB = min(512, T)
    EB = 128
    most = (n - 1) * Dn
    most_at = jnp.where(f == n - 1, Dn, 0)
    last_at = jnp.where(f == n - 1, 0, most)

    def gate_up_most(lo, hi):
        @pl.loop(lo, hi)
        def _(i):
            blk, cols = rows(i * MB, MB), pl.ds(pl.multiple_of(most_at, Dn), most)
            act[blk] = jnp.dot(tok[blk, cols], wg[cols], preferred_element_type=F32)
            coef[blk] = jnp.dot(tok[blk, cols], wu[cols], preferred_element_type=F32)

    def gate_up_last():
        @pl.loop(0, T // MB)
        def _(i):
            blk, cols = rows(i * MB, MB), rows(last_at, Dn)
            act[blk] += jnp.dot(tok[blk, cols], wg[cols], preferred_element_type=F32)
            coef[blk] += jnp.dot(tok[blk, cols], wu[cols], preferred_element_type=F32)

        @pl.loop(0, T // EB)
        def _(i):
            blk = rows(i * EB, EB)
            gate, up = act[blk], coef[blk]
            sig = jax.nn.sigmoid(gate)
            a = gate * sig
            act[blk] = a
            coef[blk] = up * sig * (1.0 + gate * (1.0 - sig))
            hT[:, blk] = (a * up).astype(BF16).T

    def hidden_most():
        @pl.loop(0, T // MB)
        def _(i):
            blk, cols = rows(i * MB, MB), pl.ds(pl.multiple_of(most_at, Dn), most)
            dh[blk] = contract_last(cot[blk, cols], wd[:, cols])

    def hidden_last():
        @pl.loop(0, T // MB)
        def _(i):
            blk, cols = rows(i * MB, MB), rows(last_at, Dn)
            dh[blk] += contract_last(cot[blk, cols], wd[:, cols])

        @pl.loop(0, T // EB)
        def _(i):
            blk = rows(i * EB, EB)
            slot, within = lax.div(i, R // EB), lax.rem(i, R // EB)
            by_core = rows((lax.rem(slot, 2) * tps + lax.div(slot, 2)) * R + within * EB, EB)
            dhid = dh[blk]
            a = (dhid * coef[blk]).astype(BF16)
            b = (dhid * act[blk]).astype(BF16)
            dg[by_core] = a
            du[by_core] = b
            gT[:, blk] = a.T
            uT[:, blk] = b.T

    sources = {DOWN: (hT, cot), GATE: (gT, tok), UP: (uT, tok)}

    def own_part(w, d):
        lhs, rhs = sources[w]
        own[...] = jnp.dot(lhs[...], rhs[:, rows(d * Dn, Dn)], preferred_element_type=F32)

    strip = H // cuts

    def strips(ref, w, k, q):
        return ref.at[w, k, pl.ds(q * strip, strip)]

    def grad_send(w, d, q, there, to):
        remote(strips(rs, w, d, q), strips(rs, w, there, q), rs_send.at[w, d, q],
               rs_recv.at[w, there, q], to).start()

    def grad_add(w, k, q):
        arrived(strips(rs, w, k, q), rs_recv.at[w, k, q])
        return own[pl.ds(q * strip, strip)] + rs[w, k, pl.ds(q * strip, strip)].astype(F32)

    def grad_edge(w, d):
        @pl.when(jnp.where(f == 0, d > 0, jnp.logical_and(f == n - 1, d < n - 1)))
        def _():
            own_part(w, d)
            rs[w, d] = own[...].astype(BF16)
            there = jnp.where(jnp.logical_and(f > 0, d == f - 1), n, d)
            to = (r, jnp.where(f == 0, 1, n - 2), t)
            for q in range(cuts):
                grad_send(w, d, q, there, to)

    def grad_edge_group(w, g):
        per = n // groups

        @pl.loop(0, per)
        def _(i):
            grad_edge(w, g * per + jnp.where(f == 0, per - 1 - i, i))

    def grad_edges(w, first, last):
        @pl.loop(first, last)
        def _(i):
            grad_edge(w, jnp.where(f == 0, n - 1 - i, i))

    def grad_through(w, dist, far):
        onward = jnp.where((2 * f < n) == (not far), 1, -1)
        d = f + dist * onward
        here = jnp.logical_and(d >= 0, d < n)

        @pl.when(jnp.logical_and(here, jnp.logical_and(f > 0, f < n - 1)))
        def _():
            own_part(w, d)
            there = jnp.where(jnp.logical_and(onward < 0, d == f - 1), n, d)
            for q in range(cuts):
                rs[w, d, pl.ds(q * strip, strip)] = grad_add(w, d, q).astype(BF16)
                grad_send(w, d, q, there, (r, f + onward, t))

    def grad_through_far(w):
        if n > 3:
            @pl.loop(0, n - 3)
            def _(i):
                for far in (False, True):
                    grad_through(w, n - 2 - i, far)

    def grad_through_near(w, far):
        if n > 2:
            grad_through(w, 1, far)

    def grads_sent(w):
        @pl.loop(0, n)
        def _(d):
            @pl.when(d != f)
            def _():
                for q in range(cuts):
                    remote(strips(rs, w, d, q), strips(rs, w, d, q), rs_send.at[w, d, q],
                           rs_recv.at[w, d, q], right).wait_send()

    def grad_final(w):
        own_part(w, f)
        for q in range(cuts):
            @pl.when(f > 0)
            def _():
                own[pl.ds(q * strip, strip)] = grad_add(w, f, q)

            @pl.when(f < n - 1)
            def _():
                own[pl.ds(q * strip, strip)] = grad_add(w, n, q)

            xs[w, pl.ds(q * strip, strip)] = own[pl.ds(q * strip, strip)].astype(BF16)
            send(xs.at[w, pl.ds(q * strip, strip)], xr.at[w, pl.ds(q * strip, strip)],
                 x_send.at[w, q], x_recv.at[w, q], x_dev)

    def halves_arrived(w):
        for q in range(cuts):
            arrived(xr.at[w, pl.ds(q * strip, strip)], x_recv.at[w, q])

    KB = min(512, D)
    at_of = lambda rr, yy: rr * ny + yy

    def product(core, first, count, put):
        blk = pl.ds(pl.multiple_of((core * 2 * ny + first) * R, R), count * R)

        @pl.loop(0, D // KB)
        def _(k):
            cols = rows(k * KB, KB)
            put(cols, contract_last(dg[blk], wg[cols]) + contract_last(du[blk], wu[cols]))

    def block(ref, rr, dy):
        return ref.at[rows(at_of(rr, yat(dy)) * R, R)]

    def tokens_for_core(rr):
        blk = rows(rr * ny * R, ny * R)

        def put(cols, value):
            pc_s[blk, cols] = value.astype(BF16)
        product(1 - c, rr * ny, ny, put)
        for dy in list(others) + [0]:
            i = at_of(rr, yat(dy))
            send(block(pc_s, rr, dy), block(pc_r, rr, dy), pc_ss.at[i], pc_rs.at[i], core_dev)

    def tokens_own(rr, dys):
        for dy in dys:
            arrived(block(pc_r, rr, dy), pc_rs.at[at_of(rr, yat(dy))])
        groups_of = [(rr * ny, ny)] if len(dys) == ny else [(at_of(rr, yat(dy)), 1) for dy in dys]
        for first, count in groups_of:
            blk = pl.ds(pl.multiple_of(first * R, R), count * R)

            def put(cols, value):
                pc_r[blk, cols] = (value + pc_r[blk, cols].astype(F32)).astype(BF16)
            product(c, first, count, put)

    quarter = R // 4
    spans = [(k * quarter, quarter) for k in range(4)]
    EC = R // 8

    def span_at(ref, span):
        return ref.at[pl.ds(span[0], span[1])]

    def add_span(rr, dy, span, refs):
        start = at_of(rr, yat(dy)) * R + span[0]

        @pl.loop(0, span[1] // EC)
        def _(k):
            here = rows(start + k * EC, EC)
            total = pc_r[here].astype(F32)
            for ref in refs:
                total += ref[rows(span[0] + k * EC, EC)].astype(F32)
            pc_r[here] = total.astype(BF16)

    def to_y(rr, which, dy, span, k):
        send(span_at(block(pc_r, rr, dy), span), span_at(py_r.at[which, dy - 1], span),
             py_ss.at[which, dy - 1, k], py_rs.at[which, dy - 1, k], y_dev(dy))

    def from_y(which, dy, span, k):
        arrived(span_at(py_r.at[which, dy - 1], span), py_rs.at[which, dy - 1, k])

    def to_x(k):
        send(span_at(block(pc_r, 1 - r, 0), spans[k]), span_at(px_r, spans[k]), px_ss.at[k], px_rs.at[k], x_dev)

    def y_out(rr, which):
        for k, span in enumerate(spans):
            for dy in others:
                to_y(rr, which, dy, span, k)

    def x_piece(k):
        for dy in others:
            from_y(0, dy, spans[k], k)
        add_span(1 - r, 0, spans[k], [py_r.at[0, dy - 1] for dy in others])
        to_x(k)

    def tokens_final():
        for k, span in enumerate(spans):
            arrived(span_at(px_r, span), px_rs.at[k])
            for dy in others:
                from_y(1, dy, span, k)
        add_span(r, 0, (0, R), [px_r] + [py_r.at[1, dy - 1] for dy in others])
        put_out(block(pc_r, r, 0), gt_out, 0)

    def squares(value):
        return jnp.sum(value * value, axis=0, keepdims=True)

    outs = []

    def put_out(src, dst, k):
        copy = pltpu.make_async_copy(src, dst, out_sem.at[k])
        copy.start()
        outs.append(copy)

    def turn(w, k, buf, at, out):
        turned[w - 1, k] = buf[w].astype(F32).T.astype(BF16)
        dst = out.at[:, rows(at * H, H)] if sliced else out.at[at]
        put_out(turned.at[w - 1, k], dst, 2 * w + k + 1)

    def wide_mine(w, out):
        tnorm[mine, pl.ds(w - 1, 1)] = squares(xs[w].astype(F32))
        turn(w, 0, xs, r, out)

    def wide_theirs(w, out):
        halves_arrived(w)
        turn(w, 1, xr, 1 - r, out)

    def wide_norms_out():
        for i in range(2):
            for k in range(tps):
                if i or k:
                    to = (r if i == 0 else 1 - r, f, lax.rem(t + k, tps))
                    at = i * tps + k
                    send(tnorm.at[mine], tnorm.at[mine], tn_ss.at[at], tn_rs.at[mine], to)

    def wide_norms_in():
        for i in range(2):
            for k in range(tps):
                if i or k:
                    slot = slot_of(r if i == 0 else 1 - r, lax.rem(t + k, tps))
                    arrived(tnorm.at[slot], tn_rs.at[slot])
        t_sum[...] = jnp.sum(tnorm[...], axis=0)
        put_out(t_sum, tn_out, 7)

    def finish_down():
        for k, (buf, at) in enumerate(((xs, r), (xr, 1 - r))):
            if k:
                halves_arrived(DOWN)
            put_out(buf.at[DOWN], gd_out.at[at], k + 1)
            fnorm[f, pl.ds(at, 1)] = squares(buf[DOWN].astype(F32).T)

    def norms_out(table, me, count, ss, rsem, dev):
        for i in range(1, count):
            send(table.at[me], table.at[me], ss.at[i - 1], rsem.at[me], dev(i))

    def norms_in(table, me, count, rsem, out):
        for i in range(1, count):
            k = lax.rem(me + i, count)
            arrived(table.at[k], rsem.at[k])
        f_sum[...] = jnp.sum(table[...], axis=0)
        put_out(f_sum, out, 8)

    order = [jnp.where(2 * f < n, groups - 1 - g, g) for g in range(groups)]

    for load in loads[:3]:
        load.wait()
    tok_out(1, 0)
    weights_step(GATE, 0)
    weights_step(UP, 0)
    tok_out(0, 1)
    for h in (0, 1):
        send_piece(*tok_piece(mine, h), core_dev)
    for load in loads[3:]:
        load.wait()
    for g in order:
        send_piece(*cot_piece(mine, g, None), core_dev)
    tnorm[mine] = jnp.zeros(tnorm.shape[1:], F32)
    fnorm[f] = jnp.zeros(fnorm.shape[1:], F32)
    if n > 2:
        weights_step(GATE, 1)
    tok_first()
    cot_out(order[0])
    tok_first_core()
    if n > 2:
        weights_step(UP, 1)
    tok_second()
    if groups > 1:
        cot_out(order[1])
    for s in range(2, n - 1):
        weights_step(GATE, s)
        weights_step(UP, s)
    weights_step(DOWN, 0)
    tok_diagonal()
    tok_from_core()
    steps = T // MB
    gate_up_most(0, steps // 2)

    def cot_next(k):
        cot_first(order[k])
        if k + 2 < groups:
            cot_out(order[k + 2])
        cot_first_core(order[k])

    cot_next(0)
    gate_up_most(steps // 2, steps)
    if groups > 1:
        cot_next(1)
    weights_step(GATE, n - 1)
    weights_step(UP, n - 1)
    cot_diagonal(order[0])
    gate_up_last()
    if groups > 2:
        cot_next(2)
    cot_from_core(order[0])
    grad_edge_group(DOWN, order[0])
    down_steps = list(range(1, n - 1))
    for s in down_steps[:1]:
        weights_step(DOWN, s)
    for k in range(1, groups):
        cot_diagonal(order[k])
        if k + 2 < groups:
            cot_next(k + 2)
        cot_from_core(order[k])
        grad_edge_group(DOWN, order[k])
        if n == 4 and k == groups - 2:
            grad_through_far(DOWN)
        for s in down_steps[k:k + 1]:
            weights_step(DOWN, s)
    for s in down_steps[groups:]:
        weights_step(DOWN, s)
    if n != 4:
        grad_through_far(DOWN)
    hidden_most()
    weights_step(DOWN, n - 1)
    hidden_last()
    grad_edges(GATE, 0, 1)
    grad_through_near(DOWN, False)
    grad_through_near(DOWN, True)
    tokens_for_core(1 - r)
    grad_edges(GATE, 1, n - 1)
    tokens_for_core(r)
    tokens_own(1 - r, list(others))
    y_out(1 - r, 0)
    grad_final(DOWN)
    grad_through_far(GATE)
    tokens_own(1 - r, [0])
    tokens_own(r, list(range(ny)))
    y_out(r, 1)
    grad_edges(UP, 0, n - 1)
    grad_through_near(GATE, False)
    x_piece(0)
    finish_down()
    norms_out(fnorm, f, n, fn_ss, fn_rs, lambda i: (r, lax.rem(f + i, n), t))
    grad_through_near(GATE, True)
    x_piece(1)
    x_piece(2)
    grad_final(GATE)
    x_piece(3)
    wide_mine(GATE, gg_out)
    grad_through_far(UP)
    grad_through_near(UP, False)
    grad_through_near(UP, True)
    wide_theirs(GATE, gg_out)
    grad_final(UP)
    wide_mine(UP, gu_out)
    wide_norms_out()
    tokens_final()
    wide_theirs(UP, gu_out)
    norms_in(fnorm, f, n, fn_rs, fn_out)
    wide_norms_in()

    for copy in outs:
        copy.wait()
    for copy in pending:
        copy.wait_send()
    for w in (DOWN, GATE, UP):
        weights_sent(w)
        grads_sent(w)


def widen(gt, gg, gu, gd, tn, fn, gt_out, gg_out, gu_out, gd_out, g_norm, u_norm, d_norm):
    gt_out[...] = gt[...]
    for src, dst in ((gg, gg_out), (gu, gu_out), (gd, gd_out)):
        dst[...] = src[...].astype(F32)
    g_norm[...] = tn[0:1]
    u_norm[...] = tn[1:2]
    if len(d_norm.shape) == 1:
        size = fn.shape[1]
        d_norm[0:size] = fn[0]
        d_norm[size:] = fn[1]
    else:
        d_norm[...] = fn[0:2]


def local(tokens, cotangent, gate_weight, up_weight, down_weight):
    n, tps = lax.axis_size("fs"), lax.axis_size("tp")
    ny = tps // 2
    R, D = tokens.shape
    H = gate_weight.shape[1] // 2
    T, Dn = 2 * tps * R, D // n
    sliced = H % 128 == 0
    if not sliced:
        r = lax.axis_index("rep")
        gate_weight = lax.dynamic_slice_in_dim(gate_weight, r * H, H, 1)
        up_weight = lax.dynamic_slice_in_dim(up_weight, r * H, H, 1)
        down_weight = lax.dynamic_slice_in_dim(down_weight, r * H, H, 0)
    blocks = 2 * tps
    groups, cuts = min(n, 4), 4
    wide_shape = (Dn, 2 * H) if sliced else (2, Dn, H)
    more = max(ny - 1, 1)
    vmem = pltpu.VMEM
    dma = lambda *shape: pltpu.SemaphoreType.DMA(shape)
    shape = jax.ShapeDtypeStruct
    any_spec = pl.BlockSpec(memory_space=pl.ANY)
    flops = 2 * 8 * T * D * H
    gt, gg, gu, gd, tn, fn = pl.pallas_call(
        functools.partial(kernel, n, tps, sliced, groups, cuts),
        out_shape=(
            shape((R, D), BF16), shape(wide_shape, BF16), shape(wide_shape, BF16),
            shape((2, H, Dn), BF16), shape((8, Dn), F32), shape((8, H), F32)),
        in_specs=[any_spec] * 5,
        out_specs=(any_spec,) * 6,
        scratch_shapes=[
            vmem((T, D), BF16), vmem((T, D), BF16),
            vmem((D, H), BF16), vmem((D, H), BF16), vmem((H, D), BF16),
            vmem((T, H), F32), vmem((T, H), F32), vmem((T, H), F32),
            vmem((H, T), BF16), vmem((H, T), BF16), vmem((H, T), BF16),
            vmem((T, H), BF16), vmem((T, H), BF16), vmem((H, Dn), F32),
            vmem((3, n + 1, H, Dn), BF16), vmem((3, H, Dn), BF16), vmem((3, H, Dn), BF16),
            vmem((2 * ny * R, D), BF16), vmem((2 * ny * R, D), BF16),
            vmem((2, more, R, D), BF16), vmem((R, D), BF16),
            vmem((2, 2, Dn, H), BF16), vmem((blocks, 8, Dn), F32), vmem((n, 8, H), F32), vmem((8, Dn), F32), vmem((8, H), F32),
            dma(5), dma(12 * ny * (groups + 1)), dma(blocks, 2), dma(blocks, groups, 2),
            dma(3, 2, n), dma(3, n), dma(3, n, cuts), dma(3, n + 1, cuts), dma(3, cuts), dma(3, cuts),
            dma(2 * ny), dma(2 * ny), dma(2, more, 4), dma(2, more, 4), dma(4), dma(4),
            dma(blocks), dma(blocks), dma(n), dma(n), dma(9),
        ],
        compiler_params=pltpu.CompilerParams(
            collective_id=0, has_side_effects=True, vmem_limit_bytes=67043328),
        cost_estimate=pl.CostEstimate(flops=flops, bytes_accessed=16 << 20, transcendentals=T * H),
    )(tokens, cotangent, gate_weight, up_weight, down_weight)
    if not sliced:
        gg, gu = (jnp.concatenate([part[0], part[1]], axis=1) for part in (gg, gu))
    steps = 2
    pieces = [(R, D), (Dn, 2 * H), (Dn, 2 * H), (2 * H, Dn)]
    tiles = [pl.BlockSpec((rows // steps, cols), lambda i: (i, 0)) for rows, cols in pieces]
    whole = lambda *dims: pl.BlockSpec(dims, lambda i: (0,) * len(dims))
    norms = [(1, Dn), (1, Dn), (2 * H,) if sliced else (2, H)]
    outs = pl.pallas_call(
        widen,
        grid=(steps,),
        out_shape=[shape(piece, F32 if i else BF16) for i, piece in enumerate(pieces)]
        + [shape(norm, F32) for norm in norms],
        in_specs=tiles + [whole(8, Dn), whole(8, H)],
        out_specs=tiles + [whole(*norm) for norm in norms],
    )(gt, gg, gu, gd.reshape(2 * H, Dn), tn, fn)
    return tuple(outs[:4]) + tuple(out.reshape(-1) for out in outs[4:])


def solution(mesh):
    placed = (
        P(("rep", "fs", "tp"), None),
        P(("rep", "fs", "tp"), None),
        P("fs", "tp"),
        P("fs", "tp"),
        P("tp", "fs"),
    )
    return jax.shard_map(
        local,
        mesh=mesh,
        in_specs=placed,
        out_specs=(
            P(("rep", "fs", "tp"), None),
            P("fs", "tp"),
            P("fs", "tp"),
            P("tp", "fs"),
            P("fs"),
            P("fs"),
            P("tp"),
        ),
        check_vma=False,
    )
```

```python
import functools

import jax
import jax.numpy as jnp
from jax import lax
from jax.experimental import pallas as pl
from jax.experimental.pallas import tpu as pltpu
from jax.sharding import PartitionSpec as P

F32, BF16 = jnp.float32, jnp.bfloat16
MESH = pl.DeviceIdType.MESH
DOWN, GATE, UP = 0, 1, 2


def contract_last(left, right):
    return lax.dot_general(
        left, right, (((1,), (1,)), ((), ())), preferred_element_type=F32
    )


def kernel(n, tps, sliced, groups, cuts, tok_in, cot_in, wg_in, wu_in, wd_in,
           gt_out, gg_out, gu_out, gd_out, tn_out, fn_out,
           tok, cot, wg, wu, wd, act, coef, dh, hT, gT, uT, dg, du, own, rs, xs, xr,
           pc_s, pc_r, py_r, px_r, turned, tnorm, fnorm, t_sum, f_sum,
           load_sem, ag_send, tok_recv, cot_recv, z_send, z_recv, rs_send, rs_recv,
           x_send, x_recv, pc_ss, pc_rs, py_ss, py_rs, px_ss, px_rs,
           tn_ss, tn_rs, fn_ss, fn_rs, out_sem):
    ny = tps // 2
    r, f, t = lax.axis_index("rep"), lax.axis_index("fs"), lax.axis_index("tp")
    y, c = lax.div(t, 2), lax.rem(t, 2)
    R, D = tok_in.shape
    T, H = tok.shape[0], wg.shape[1]
    Dn, half_rows, chunk = D // n, R // 2, D // groups
    tcore = t + 1 - 2 * c
    core_dev, x_dev = (r, f, tcore), (1 - r, f, t)
    yat = lambda dy: lax.rem(y + dy + ny, ny)
    ty = lambda dy: yat(dy) * 2 + c
    y_dev = lambda dy: (r, f, ty(dy))
    right, left = (r, lax.rem(f + 1, n), t), (r, lax.rem(f + n - 1, n), t)
    others = range(1, ny)

    def remote(src, dst, ss, rsem, dev):
        return pltpu.make_async_remote_copy(
            src_ref=src, dst_ref=dst, send_sem=ss, recv_sem=rsem,
            device_id=dev, device_id_type=MESH)

    def arrived(dst, sem):
        remote(dst, dst, sem, sem, core_dev).wait_recv()

    def rows(start, size):
        return pl.ds(pl.multiple_of(start, size), size)

    def send(*args):
        remote(*args).start()

    def all_sent(view, sem):
        remote(view, view, sem, sem, core_dev).wait_send()

    half = (lambda ref: ref.at[:, rows(r * H, H)]) if sliced else (lambda ref: ref)
    half_d = (lambda ref: ref.at[rows(r * H, H)]) if sliced else (lambda ref: ref)
    my_rows = rows((r * tps + t) * R, R)
    loads = [
        pltpu.make_async_copy(src, dst, load_sem.at[i]) for i, (src, dst) in enumerate([
            (tok_in, tok.at[my_rows]),
            (half(wg_in), wg.at[rows(f * Dn, Dn)]),
            (half(wu_in), wu.at[rows(f * Dn, Dn)]),
            (cot_in, cot.at[my_rows]),
            (half_d(wd_in), wd.at[:, rows(f * Dn, Dn)]),
        ])]
    for load in loads:
        load.start()

    barrier = pltpu.get_barrier_semaphore()
    for i in range(1, tps):
        pl.semaphore_signal(barrier, inc=1, device_id=(r, f, lax.rem(t + i, tps)), device_id_type=MESH)
    for i in range(1, n):
        pl.semaphore_signal(barrier, inc=1, device_id=(r, lax.rem(f + i, n), t), device_id_type=MESH)
    for i in range(tps):
        pl.semaphore_signal(barrier, inc=1, device_id=(1 - r, f, lax.rem(t + i, tps)), device_id_type=MESH)
    pl.semaphore_wait(barrier, tps - 1 + n - 1 + tps)

    sent = [0, 0]

    def send_piece(view, sem, dev, a=0):
        send(view, view, ag_send.at[a], sem, dev)
        sent[a] += view.shape[0] * view.shape[1]

    slot_of = lambda rr, tt: rr * tps + tt

    def tok_piece(slot, h):
        return tok.at[rows(slot * R + h * half_rows, half_rows)], tok_recv.at[slot, h]

    def cot_piece(slot, g, h):
        at = rows(slot * R, R) if h is None else rows(slot * R + h * half_rows, half_rows)
        return cot.at[at, rows(g * chunk, chunk)], cot_recv.at[slot, g]

    mine, beside = slot_of(r, t), slot_of(1 - r, t)
    along = lambda dy: slot_of(r, ty(-dy))
    diagonal = lambda dy: slot_of(1 - r, ty(-dy))
    cored = lambda tt: tt + 1 - 2 * c

    def tok_out(to_x, to_y):
        send_piece(*tok_piece(mine, to_x), x_dev)
        for dy in others:
            send_piece(*tok_piece(mine, to_y), y_dev(dy))

    def tok_first():
        arrived(*tok_piece(beside, 1))
        for dy in others:
            send_piece(*tok_piece(beside, 1), y_dev(dy))
        for dy in others:
            arrived(*tok_piece(along(dy), 0))
            send_piece(*tok_piece(along(dy), 0), x_dev)

    def tok_first_core():
        send_piece(*tok_piece(beside, 1), core_dev)
        for dy in others:
            send_piece(*tok_piece(along(dy), 0), core_dev)

    def tok_second():
        for slot, h in [(beside, 0)] + [(along(dy), 1) for dy in others]:
            arrived(*tok_piece(slot, h))
            send_piece(*tok_piece(slot, h), core_dev)

    def tok_diagonal():
        for dy in others:
            for h in (0, 1):
                arrived(*tok_piece(diagonal(dy), h))
                send_piece(*tok_piece(diagonal(dy), h), core_dev)

    def tok_from_core():
        for dy in range(ny):
            for rr in (r, 1 - r):
                for h in (0, 1):
                    arrived(*tok_piece(slot_of(rr, cored(ty(dy))), h))

    def cot_send(slot, g, h, dev):
        send_piece(*cot_piece(slot, g, h), dev, 1)

    def cot_out(g):
        cot_send(mine, g, None, x_dev)
        for dy in others:
            cot_send(mine, g, None, y_dev(dy))

    def cot_first(g):
        arrived(*cot_piece(beside, g, None))
        for dy in others:
            cot_send(beside, g, 1, y_dev(dy))
        for dy in others:
            arrived(*cot_piece(along(dy), g, None))
            cot_send(along(dy), g, 0, x_dev)

    def cot_first_core(g):
        for slot in [beside] + [along(dy) for dy in others]:
            cot_send(slot, g, None, core_dev)

    def cot_diagonal(g):
        for dy in others:
            arrived(*cot_piece(diagonal(dy), g, None))
            cot_send(diagonal(dy), g, None, core_dev)

    def cot_from_core(g):
        for dy in range(ny):
            for rr in (r, 1 - r):
                arrived(*cot_piece(slot_of(rr, cored(ty(dy))), g, None))

    def weight(w, k):
        if w == DOWN:
            return wd.at[:, rows(k * Dn, Dn)]
        return (wg if w == GATE else wu).at[rows(k * Dn, Dn)]

    def ways(s):
        return ((0, right, f - s, f - s >= 0, f + 1 < n), (1, left, f + s, f + s < n, f > 0))

    def weights_step(w, s):
        for way, to, origin, has, sends in ways(s):
            @pl.when(has)
            def _():
                view = weight(w, origin)
                if s:
                    arrived(view, z_recv.at[w, origin])
                if s < n - 1:
                    @pl.when(sends)
                    def _():
                        remote(view, view, z_send.at[w, way, s], z_recv.at[w, origin], to).start()

    def weights_sent(w):
        for s in range(n - 1):
            for way, to, origin, has, sends in ways(s):
                @pl.when(jnp.logical_and(has, sends))
                def _():
                    view = weight(w, origin)
                    remote(view, view, z_send.at[w, way, s], z_recv.at[w, origin], to).wait_send()

    MB = min(512, T)
    EB = 128
    most = (n - 1) * Dn
    most_at = jnp.where(f == n - 1, Dn, 0)
    last_at = jnp.where(f == n - 1, 0, most)

    def gate_up_most(lo, hi):
        @pl.loop(lo, hi)
        def _(i):
            blk, cols = rows(i * MB, MB), pl.ds(pl.multiple_of(most_at, Dn), most)
            act[blk] = jnp.dot(tok[blk, cols], wg[cols], preferred_element_type=F32)
            coef[blk] = jnp.dot(tok[blk, cols], wu[cols], preferred_element_type=F32)

    def gate_up_last():
        @pl.loop(0, T // MB)
        def _(i):
            blk, cols = rows(i * MB, MB), rows(last_at, Dn)
            act[blk] += jnp.dot(tok[blk, cols], wg[cols], preferred_element_type=F32)
            coef[blk] += jnp.dot(tok[blk, cols], wu[cols], preferred_element_type=F32)

        @pl.loop(0, T // EB)
        def _(i):
            blk = rows(i * EB, EB)
            gate = act[blk]
            hT[:, blk] = (gate * jax.nn.sigmoid(gate) * coef[blk]).astype(BF16).T

    def slopes():
        @pl.loop(0, T // EB)
        def _(i):
            blk = rows(i * EB, EB)
            gate, up = act[blk], coef[blk]
            sig = jax.nn.sigmoid(gate)
            act[blk] = gate * sig
            coef[blk] = up * sig * (1.0 + gate * (1.0 - sig))

    def hidden_most():
        @pl.loop(0, T // MB)
        def _(i):
            blk, cols = rows(i * MB, MB), pl.ds(pl.multiple_of(most_at, Dn), most)
            dh[blk] = contract_last(cot[blk, cols], wd[:, cols])

    def hidden_last():
        @pl.loop(0, T // MB)
        def _(i):
            blk, cols = rows(i * MB, MB), rows(last_at, Dn)
            dh[blk] += contract_last(cot[blk, cols], wd[:, cols])

        @pl.loop(0, T // EB)
        def _(i):
            blk = rows(i * EB, EB)
            slot, within = lax.div(i, R // EB), lax.rem(i, R // EB)
            by_core = rows((lax.rem(slot, 2) * tps + lax.div(slot, 2)) * R + within * EB, EB)
            dhid = dh[blk]
            a = (dhid * coef[blk]).astype(BF16)
            b = (dhid * act[blk]).astype(BF16)
            dg[by_core] = a
            du[by_core] = b
            gT[:, blk] = a.T
            uT[:, blk] = b.T

    sources = {DOWN: (hT, cot), GATE: (gT, tok), UP: (uT, tok)}

    def own_part(w, d):
        lhs, rhs = sources[w]
        own[...] = jnp.dot(lhs[...], rhs[:, rows(d * Dn, Dn)], preferred_element_type=F32)

    strip = H // cuts

    def strips(ref, w, k, q):
        return ref.at[w, k, pl.ds(q * strip, strip)]

    def grad_send(w, d, q, there, to):
        remote(strips(rs, w, d, q), strips(rs, w, there, q), rs_send.at[w],
               rs_recv.at[w, there, q], to).start()

    def grad_add(w, k, q):
        arrived(strips(rs, w, k, q), rs_recv.at[w, k, q])
        return own[pl.ds(q * strip, strip)] + rs[w, k, pl.ds(q * strip, strip)].astype(F32)

    def grad_edge(w, d):
        @pl.when(jnp.where(f == 0, d > 0, jnp.logical_and(f == n - 1, d < n - 1)))
        def _():
            own_part(w, d)
            rs[w, d] = own[...].astype(BF16)
            there = jnp.where(jnp.logical_and(f > 0, d == f - 1), n, d)
            to = (r, jnp.where(f == 0, 1, n - 2), t)
            for q in range(cuts):
                grad_send(w, d, q, there, to)

    def grad_edge_group(w, g):
        per = n // groups

        @pl.loop(0, per)
        def _(i):
            grad_edge(w, g * per + jnp.where(f == 0, per - 1 - i, i))

    def grad_edges(w, first, last):
        @pl.loop(first, last)
        def _(i):
            grad_edge(w, jnp.where(f == 0, n - 1 - i, i))

    def grad_through(w, dist, far):
        onward = jnp.where((2 * f < n) == (not far), 1, -1)
        d = f + dist * onward
        here = jnp.logical_and(d >= 0, d < n)

        @pl.when(jnp.logical_and(here, jnp.logical_and(f > 0, f < n - 1)))
        def _():
            own_part(w, d)
            there = jnp.where(jnp.logical_and(onward < 0, d == f - 1), n, d)
            for q in range(cuts):
                rs[w, d, pl.ds(q * strip, strip)] = grad_add(w, d, q).astype(BF16)
                grad_send(w, d, q, there, (r, f + onward, t))

    def grad_through_far(w):
        if n > 3:
            @pl.loop(0, n - 3)
            def _(i):
                for far in (False, True):
                    grad_through(w, n - 2 - i, far)

    def grad_through_near(w, far):
        if n > 2:
            grad_through(w, 1, far)

    def grads_sent(w):
        all_sent(rs.at[w, pl.ds(0, n - 1)], rs_send.at[w])
        all_sent(xs.at[w], x_send.at[w])

    def grad_final(w):
        own_part(w, f)
        for q in range(cuts):
            @pl.when(f > 0)
            def _():
                own[pl.ds(q * strip, strip)] = grad_add(w, f, q)

            @pl.when(f < n - 1)
            def _():
                own[pl.ds(q * strip, strip)] = grad_add(w, n, q)

            xs[w, pl.ds(q * strip, strip)] = own[pl.ds(q * strip, strip)].astype(BF16)
            send(xs.at[w, pl.ds(q * strip, strip)], xr.at[w, pl.ds(q * strip, strip)],
                 x_send.at[w], x_recv.at[w], x_dev)

    def halves_arrived(w):
        arrived(xr.at[w], x_recv.at[w])

    KB = min(512, D)
    at_of = lambda rr, yy: rr * ny + yy

    def product(core, first, count, put):
        blk = pl.ds(pl.multiple_of((core * 2 * ny + first) * R, R), count * R)

        @pl.loop(0, D // KB)
        def _(k):
            cols = rows(k * KB, KB)
            put(cols, contract_last(dg[blk], wg[cols]) + contract_last(du[blk], wu[cols]))

    def block(ref, rr, dy):
        return ref.at[rows(at_of(rr, yat(dy)) * R, R)]

    def tokens_for_core(rr):
        blk = rows(rr * ny * R, ny * R)

        def put(cols, value):
            pc_s[blk, cols] = value.astype(BF16)
        product(1 - c, rr * ny, ny, put)
        for dy in list(others) + [0]:
            i = at_of(rr, yat(dy))
            send(block(pc_s, rr, dy), block(pc_r, rr, dy), pc_ss, pc_rs.at[i], core_dev)

    def tokens_own(rr, dys):
        for dy in dys:
            arrived(block(pc_r, rr, dy), pc_rs.at[at_of(rr, yat(dy))])
        groups_of = [(rr * ny, ny)] if len(dys) == ny else [(at_of(rr, yat(dy)), 1) for dy in dys]
        for first, count in groups_of:
            blk = pl.ds(pl.multiple_of(first * R, R), count * R)

            def put(cols, value):
                pc_r[blk, cols] = (value + pc_r[blk, cols].astype(F32)).astype(BF16)
            product(c, first, count, put)

    quarter = R // 4
    spans = [(k * quarter, quarter) for k in range(4)]
    EC = R // 8

    def span_at(ref, span):
        return ref.at[pl.ds(span[0], span[1])]

    def add_span(rr, dy, span, refs):
        start = at_of(rr, yat(dy)) * R + span[0]

        @pl.loop(0, span[1] // EC)
        def _(k):
            here = rows(start + k * EC, EC)
            total = pc_r[here].astype(F32)
            for ref in refs:
                total += ref[rows(span[0] + k * EC, EC)].astype(F32)
            pc_r[here] = total.astype(BF16)

    def to_y(rr, which, dy, span, k):
        send(span_at(block(pc_r, rr, dy), span), span_at(py_r.at[which, dy - 1], span),
             py_ss.at[which], py_rs.at[which, dy - 1, k], y_dev(dy))

    def from_y(which, dy, span, k):
        arrived(span_at(py_r.at[which, dy - 1], span), py_rs.at[which, dy - 1, k])

    def to_x(k):
        send(span_at(block(pc_r, 1 - r, 0), spans[k]), span_at(px_r, spans[k]), px_ss, px_rs.at[k], x_dev)

    def y_out(rr, which):
        for k, span in enumerate(spans):
            for dy in others:
                to_y(rr, which, dy, span, k)

    def x_piece(k):
        for dy in others:
            from_y(0, dy, spans[k], k)
        add_span(1 - r, 0, spans[k], [py_r.at[0, dy - 1] for dy in others])
        to_x(k)

    def tokens_final():
        for k, span in enumerate(spans):
            arrived(span_at(px_r, span), px_rs.at[k])
            for dy in others:
                from_y(1, dy, span, k)
        add_span(r, 0, (0, R), [px_r] + [py_r.at[1, dy - 1] for dy in others])
        put_out(block(pc_r, r, 0), gt_out, 0)

    def squares(value):
        return jnp.sum(value * value, axis=0, keepdims=True)

    outs = []

    def put_out(src, dst, k):
        copy = pltpu.make_async_copy(src, dst, out_sem.at[k])
        copy.start()
        outs.append(copy)

    def turn(w, k, buf, at, out):
        turned[w - 1, k] = buf[w].astype(F32).T.astype(BF16)
        dst = out.at[:, rows(at * H, H)] if sliced else out.at[at]
        put_out(turned.at[w - 1, k], dst, 2 * w + k + 1)

    def wide_mine(w, out):
        tnorm[mine, pl.ds(w - 1, 1)] = squares(xs[w].astype(F32))
        turn(w, 0, xs, r, out)

    def wide_theirs(w, out):
        halves_arrived(w)
        turn(w, 1, xr, 1 - r, out)

    def wide_norms_out():
        for i in range(2):
            for k in range(tps):
                if i or k:
                    to = (r if i == 0 else 1 - r, f, lax.rem(t + k, tps))
                    send(tnorm.at[mine], tnorm.at[mine], tn_ss, tn_rs, to)

    def wide_norms_in():
        arrived(tnorm.at[pl.ds(0, 2 * tps - 1)], tn_rs)
        t_sum[...] = jnp.sum(tnorm[...], axis=0)
        put_out(t_sum, tn_out, 7)

    def finish_down():
        for k, (buf, at) in enumerate(((xs, r), (xr, 1 - r))):
            if k:
                halves_arrived(DOWN)
            put_out(buf.at[DOWN], gd_out.at[at], k + 1)
            fnorm[f, pl.ds(at, 1)] = squares(buf[DOWN].astype(F32).T)

    def norms_out():
        for i in range(1, n):
            send(fnorm.at[f], fnorm.at[f], fn_ss, fn_rs, (r, lax.rem(f + i, n), t))

    def norms_in():
        arrived(fnorm.at[pl.ds(0, n - 1)], fn_rs)
        f_sum[...] = jnp.sum(fnorm[...], axis=0)
        put_out(f_sum, fn_out, 8)

    order = [jnp.where(2 * f < n, groups - 1 - g, g) for g in range(groups)]

    for load in loads[:3]:
        load.wait()
    tok_out(1, 0)
    weights_step(GATE, 0)
    weights_step(UP, 0)
    tok_out(0, 1)
    for h in (0, 1):
        send_piece(*tok_piece(mine, h), core_dev)
    for load in loads[3:]:
        load.wait()
    for g in order:
        cot_send(mine, g, None, core_dev)
    tnorm[mine] = jnp.zeros(tnorm.shape[1:], F32)
    fnorm[f] = jnp.zeros(fnorm.shape[1:], F32)
    if n > 2:
        weights_step(GATE, 1)
    tok_first()
    cot_out(order[0])
    tok_first_core()
    if n > 2:
        weights_step(UP, 1)
    tok_second()
    if groups > 1:
        cot_out(order[1])
    for s in range(2, n - 1):
        weights_step(GATE, s)
        weights_step(UP, s)
    weights_step(DOWN, 0)
    tok_diagonal()
    tok_from_core()
    steps = T // MB
    gate_up_most(0, steps // 2)

    def cot_next(k):
        cot_first(order[k])
        if k + 2 < groups:
            cot_out(order[k + 2])
        cot_first_core(order[k])

    cot_next(0)
    gate_up_most(steps // 2, steps)
    if groups > 1:
        cot_next(1)
    weights_step(GATE, n - 1)
    weights_step(UP, n - 1)
    cot_diagonal(order[0])
    gate_up_last()
    if groups > 2:
        cot_next(2)
    cot_from_core(order[0])
    grad_edge_group(DOWN, order[0])
    slopes()
    down_steps = list(range(1, n - 1))
    for s in down_steps[:1]:
        weights_step(DOWN, s)
    for k in range(1, groups):
        cot_diagonal(order[k])
        if k + 2 < groups:
            cot_next(k + 2)
        cot_from_core(order[k])
        grad_edge_group(DOWN, order[k])
        if n == 4 and k == groups - 2:
            grad_through_far(DOWN)
        for s in down_steps[k:k + 1]:
            weights_step(DOWN, s)
    for s in down_steps[groups:]:
        weights_step(DOWN, s)
    if n != 4:
        grad_through_far(DOWN)
    hidden_most()
    weights_step(DOWN, n - 1)
    hidden_last()
    grad_edges(GATE, 0, 1)
    grad_through_near(DOWN, False)
    grad_through_near(DOWN, True)
    tokens_for_core(1 - r)
    grad_edges(GATE, 1, n - 1)
    tokens_for_core(r)
    tokens_own(1 - r, list(others))
    y_out(1 - r, 0)
    grad_final(DOWN)
    grad_through_far(GATE)
    tokens_own(1 - r, [0])
    tokens_own(r, list(range(ny)))
    y_out(r, 1)
    grad_edges(UP, 0, n - 1)
    grad_through_near(GATE, False)
    x_piece(0)
    finish_down()
    norms_out()
    grad_through_near(GATE, True)
    x_piece(1)
    x_piece(2)
    grad_final(GATE)
    x_piece(3)
    wide_mine(GATE, gg_out)
    grad_through_far(UP)
    grad_through_near(UP, False)
    grad_through_near(UP, True)
    wide_theirs(GATE, gg_out)
    grad_final(UP)
    wide_mine(UP, gu_out)
    wide_norms_out()
    tokens_final()
    wide_theirs(UP, gu_out)
    norms_in()
    wide_norms_in()

    for copy in outs:
        copy.wait()
    for a, buf in enumerate((tok, cot)):
        all_sent(buf.at[pl.ds(0, sent[a] // D)], ag_send.at[a])
    for w in (DOWN, GATE, UP):
        weights_sent(w)
        grads_sent(w)
    all_sent(pc_s, pc_ss)
    if ny > 1:
        for which in (0, 1):
            all_sent(py_r.at[which], py_ss.at[which])
    all_sent(px_r, px_ss)
    all_sent(tnorm.at[pl.ds(0, 2 * tps - 1)], tn_ss)
    all_sent(fnorm.at[pl.ds(0, n - 1)], fn_ss)


def widen(gt, gg, gu, gd, tn, fn, gt_out, gg_out, gu_out, gd_out, g_norm, u_norm, d_norm):
    gt_out[...] = gt[...]
    for src, dst in ((gg, gg_out), (gu, gu_out), (gd, gd_out)):
        dst[...] = src[...].astype(F32)
    g_norm[...] = tn[0:1]
    u_norm[...] = tn[1:2]
    if len(d_norm.shape) == 1:
        size = fn.shape[1]
        d_norm[0:size] = fn[0]
        d_norm[size:] = fn[1]
    else:
        d_norm[...] = fn[0:2]


def local(tokens, cotangent, gate_weight, up_weight, down_weight):
    n, tps = lax.axis_size("fs"), lax.axis_size("tp")
    ny = tps // 2
    R, D = tokens.shape
    H = gate_weight.shape[1] // 2
    T, Dn = 2 * tps * R, D // n
    sliced = H % 128 == 0
    if not sliced:
        r = lax.axis_index("rep")
        gate_weight = lax.dynamic_slice_in_dim(gate_weight, r * H, H, 1)
        up_weight = lax.dynamic_slice_in_dim(up_weight, r * H, H, 1)
        down_weight = lax.dynamic_slice_in_dim(down_weight, r * H, H, 0)
    blocks = 2 * tps
    groups, cuts = min(n, 4), 4
    wide_shape = (Dn, 2 * H) if sliced else (2, Dn, H)
    more = max(ny - 1, 1)
    vmem = pltpu.VMEM
    one = pltpu.SemaphoreType.DMA
    dma = lambda *shape: one(shape)
    shape = jax.ShapeDtypeStruct
    any_spec = pl.BlockSpec(memory_space=pl.ANY)
    flops = 2 * 8 * T * D * H
    gt, gg, gu, gd, tn, fn = pl.pallas_call(
        functools.partial(kernel, n, tps, sliced, groups, cuts),
        out_shape=(
            shape((R, D), BF16), shape(wide_shape, BF16), shape(wide_shape, BF16),
            shape((2, H, Dn), BF16), shape((8, Dn), F32), shape((8, H), F32)),
        in_specs=[any_spec] * 5,
        out_specs=(any_spec,) * 6,
        scratch_shapes=[
            vmem((T, D), BF16), vmem((T, D), BF16),
            vmem((D, H), BF16), vmem((D, H), BF16), vmem((H, D), BF16),
            vmem((T, H), F32), vmem((T, H), F32), vmem((T, H), F32),
            vmem((H, T), BF16), vmem((H, T), BF16), vmem((H, T), BF16),
            vmem((T, H), BF16), vmem((T, H), BF16), vmem((H, Dn), F32),
            vmem((3, n + 1, H, Dn), BF16), vmem((3, H, Dn), BF16), vmem((3, H, Dn), BF16),
            vmem((2 * ny * R, D), BF16), vmem((2 * ny * R, D), BF16),
            vmem((2, more, R, D), BF16), vmem((R, D), BF16),
            vmem((2, 2, Dn, H), BF16), vmem((blocks, 8, Dn), F32), vmem((n, 8, H), F32), vmem((8, Dn), F32), vmem((8, H), F32),
            dma(5), dma(2), dma(blocks, 2), dma(blocks, groups),
            dma(3, 2, n - 1), dma(3, n), dma(3), dma(3, n + 1, cuts), dma(3), dma(3),
            one, dma(2 * ny), dma(2), dma(2, more, 4), one, dma(4),
            one, one, one, one, dma(9),
        ],
        compiler_params=pltpu.CompilerParams(
            collective_id=0, has_side_effects=True, vmem_limit_bytes=67043328),
        cost_estimate=pl.CostEstimate(flops=flops, bytes_accessed=16 << 20, transcendentals=T * H),
    )(tokens, cotangent, gate_weight, up_weight, down_weight)
    if not sliced:
        gg, gu = (jnp.concatenate([part[0], part[1]], axis=1) for part in (gg, gu))
    steps = 2
    pieces = [(R, D), (Dn, 2 * H), (Dn, 2 * H), (2 * H, Dn)]
    tiles = [pl.BlockSpec((rows // steps, cols), lambda i: (i, 0)) for rows, cols in pieces]
    whole = lambda *dims: pl.BlockSpec(dims, lambda i: (0,) * len(dims))
    norms = [(1, Dn), (1, Dn), (2 * H,) if sliced else (2, H)]
    outs = pl.pallas_call(
        widen,
        grid=(steps,),
        out_shape=[shape(piece, F32 if i else BF16) for i, piece in enumerate(pieces)]
        + [shape(norm, F32) for norm in norms],
        in_specs=tiles + [whole(8, Dn), whole(8, H)],
        out_specs=tiles + [whole(*norm) for norm in norms],
    )(gt, gg, gu, gd.reshape(2 * H, Dn), tn, fn)
    return tuple(outs[:4]) + tuple(out.reshape(-1) for out in outs[4:])


def solution(mesh):
    placed = (
        P(("rep", "fs", "tp"), None),
        P(("rep", "fs", "tp"), None),
        P("fs", "tp"),
        P("fs", "tp"),
        P("tp", "fs"),
    )
    return jax.shard_map(
        local,
        mesh=mesh,
        in_specs=placed,
        out_specs=(
            P(("rep", "fs", "tp"), None),
            P("fs", "tp"),
            P("fs", "tp"),
            P("tp", "fs"),
            P("fs"),
            P("fs"),
            P("tp"),
        ),
        check_vma=False,
    )
```

```python
import functools

import jax
import jax.numpy as jnp
from jax import lax
from jax.experimental import pallas as pl
from jax.experimental.pallas import tpu as pltpu
from jax.sharding import PartitionSpec as P

F32, BF16 = jnp.float32, jnp.bfloat16
MESH = pl.DeviceIdType.MESH
DOWN, GATE, UP = 0, 1, 2


def contract_last(left, right):
    return lax.dot_general(
        left, right, (((1,), (1,)), ((), ())), preferred_element_type=F32
    )


def kernel(n, tps, sliced, groups, cuts, tok_in, cot_in, wg_in, wu_in, wd_in,
           gt_out, gg_out, gu_out, gd_out, tn_out, fn_out,
           tok, cot, wg, wu, wd, act, coef, dh, hT, gT, uT, dg, du, own, rs, xs, xr,
           pc_s, pc_r, py_r, px_r, turned, tnorm, fnorm, t_sum, f_sum,
           load_sem, ag_send, tok_recv, cot_recv, z_send, z_recv, rs_send, rs_recv,
           x_send, x_recv, pc_ss, pc_rs, py_ss, py_rs, px_ss, px_rs,
           tn_ss, tn_rs, fn_ss, fn_rs, out_sem):
    ny = tps // 2
    r, f, t = lax.axis_index("rep"), lax.axis_index("fs"), lax.axis_index("tp")
    y, c = lax.div(t, 2), lax.rem(t, 2)
    R, D = tok_in.shape
    T, H = tok.shape[0], wg.shape[1]
    Dn, half_rows, chunk = D // n, R // 2, D // groups
    tcore = t + 1 - 2 * c
    core_dev, x_dev = (r, f, tcore), (1 - r, f, t)
    yat = lambda dy: lax.rem(y + dy + ny, ny)
    ty = lambda dy: yat(dy) * 2 + c
    y_dev = lambda dy: (r, f, ty(dy))
    right, left = (r, lax.rem(f + 1, n), t), (r, lax.rem(f + n - 1, n), t)
    others = range(1, ny)

    def remote(src, dst, ss, rsem, dev):
        return pltpu.make_async_remote_copy(
            src_ref=src, dst_ref=dst, send_sem=ss, recv_sem=rsem,
            device_id=dev, device_id_type=MESH)

    def arrived(dst, sem):
        remote(dst, dst, sem, sem, core_dev).wait_recv()

    def rows(start, size):
        return pl.ds(pl.multiple_of(start, size), size)

    def send(*args):
        remote(*args).start()

    def all_sent(view, sem):
        remote(view, view, sem, sem, core_dev).wait_send()

    half = (lambda ref: ref.at[:, rows(r * H, H)]) if sliced else (lambda ref: ref)
    half_d = (lambda ref: ref.at[rows(r * H, H)]) if sliced else (lambda ref: ref)
    my_rows = rows((r * tps + t) * R, R)
    loads = [
        pltpu.make_async_copy(src, dst, load_sem.at[i]) for i, (src, dst) in enumerate([
            (tok_in, tok.at[my_rows]),
            (half(wg_in), wg.at[rows(f * Dn, Dn)]),
            (half(wu_in), wu.at[rows(f * Dn, Dn)]),
            (cot_in, cot.at[my_rows]),
            (half_d(wd_in), wd.at[:, rows(f * Dn, Dn)]),
        ])]
    for load in loads:
        load.start()

    barrier = pltpu.get_barrier_semaphore()
    for i in range(1, tps):
        pl.semaphore_signal(barrier, inc=1, device_id=(r, f, lax.rem(t + i, tps)), device_id_type=MESH)
    for i in range(1, n):
        pl.semaphore_signal(barrier, inc=1, device_id=(r, lax.rem(f + i, n), t), device_id_type=MESH)
    for i in range(tps):
        pl.semaphore_signal(barrier, inc=1, device_id=(1 - r, f, lax.rem(t + i, tps)), device_id_type=MESH)
    pl.semaphore_wait(barrier, tps - 1 + n - 1 + tps)

    sent = [0, 0]

    def send_piece(view, sem, dev, a=0):
        send(view, view, ag_send.at[a], sem, dev)
        sent[a] += view.shape[0] * view.shape[1]

    slot_of = lambda rr, tt: rr * tps + tt

    def tok_piece(slot, h):
        return tok.at[rows(slot * R + h * half_rows, half_rows)], tok_recv.at[slot, h]

    def cot_piece(slot, g, h):
        at = rows(slot * R, R) if h is None else rows(slot * R + h * half_rows, half_rows)
        return cot.at[at, rows(g * chunk, chunk)], cot_recv.at[slot, g]

    mine, beside = slot_of(r, t), slot_of(1 - r, t)
    along = lambda dy: slot_of(r, ty(-dy))
    diagonal = lambda dy: slot_of(1 - r, ty(-dy))
    cored = lambda tt: tt + 1 - 2 * c

    def tok_out(to_x, to_y):
        send_piece(*tok_piece(mine, to_x), x_dev)
        for dy in others:
            send_piece(*tok_piece(mine, to_y), y_dev(dy))

    def tok_first():
        arrived(*tok_piece(beside, 1))
        for dy in others:
            send_piece(*tok_piece(beside, 1), y_dev(dy))
        for dy in others:
            arrived(*tok_piece(along(dy), 0))
            send_piece(*tok_piece(along(dy), 0), x_dev)

    def tok_first_core():
        send_piece(*tok_piece(beside, 1), core_dev)
        for dy in others:
            send_piece(*tok_piece(along(dy), 0), core_dev)

    def tok_second():
        for slot, h in [(beside, 0)] + [(along(dy), 1) for dy in others]:
            arrived(*tok_piece(slot, h))
            send_piece(*tok_piece(slot, h), core_dev)

    def tok_diagonal():
        for dy in others:
            for h in (0, 1):
                arrived(*tok_piece(diagonal(dy), h))
                send_piece(*tok_piece(diagonal(dy), h), core_dev)

    def tok_from_core():
        for dy in range(ny):
            for rr in (r, 1 - r):
                for h in (0, 1):
                    arrived(*tok_piece(slot_of(rr, cored(ty(dy))), h))

    def cot_send(slot, g, h, dev):
        send_piece(*cot_piece(slot, g, h), dev, 1)

    def cot_out(g):
        cot_send(mine, g, None, x_dev)
        for dy in others:
            cot_send(mine, g, None, y_dev(dy))

    def cot_first(g):
        arrived(*cot_piece(beside, g, None))
        for dy in others:
            cot_send(beside, g, 1, y_dev(dy))
        for dy in others:
            arrived(*cot_piece(along(dy), g, None))
            cot_send(along(dy), g, 0, x_dev)

    def cot_first_core(g):
        for slot in [beside] + [along(dy) for dy in others]:
            cot_send(slot, g, None, core_dev)

    def cot_diagonal(g):
        for dy in others:
            arrived(*cot_piece(diagonal(dy), g, None))
            cot_send(diagonal(dy), g, None, core_dev)

    def cot_from_core(g):
        for dy in range(ny):
            for rr in (r, 1 - r):
                arrived(*cot_piece(slot_of(rr, cored(ty(dy))), g, None))

    def weight(w, k):
        if w == DOWN:
            return wd.at[:, rows(k * Dn, Dn)]
        return (wg if w == GATE else wu).at[rows(k * Dn, Dn)]

    def ways(s):
        return ((0, right, f - s, f - s >= 0, f + 1 < n), (1, left, f + s, f + s < n, f > 0))

    def weights_step(w, s):
        for way, to, origin, has, sends in ways(s):
            @pl.when(has)
            def _():
                view = weight(w, origin)
                if s:
                    arrived(view, z_recv.at[w, origin])
                if s < n - 1:
                    @pl.when(sends)
                    def _():
                        remote(view, view, z_send.at[w, way, s], z_recv.at[w, origin], to).start()

    def weights_sent(w):
        for s in range(n - 1):
            for way, to, origin, has, sends in ways(s):
                @pl.when(jnp.logical_and(has, sends))
                def _():
                    view = weight(w, origin)
                    remote(view, view, z_send.at[w, way, s], z_recv.at[w, origin], to).wait_send()

    MB = min(512, T)
    EB = 128
    most = (n - 1) * Dn
    most_at = jnp.where(f == n - 1, Dn, 0)
    last_at = jnp.where(f == n - 1, 0, most)

    def gate_up_most(lo, hi):
        @pl.loop(lo, hi)
        def _(i):
            blk, cols = rows(i * MB, MB), pl.ds(pl.multiple_of(most_at, Dn), most)
            act[blk] = jnp.dot(tok[blk, cols], wg[cols], preferred_element_type=F32)
            coef[blk] = jnp.dot(tok[blk, cols], wu[cols], preferred_element_type=F32)

    def gate_up_last():
        @pl.loop(0, T // MB)
        def _(i):
            blk, cols = rows(i * MB, MB), rows(last_at, Dn)
            act[blk] += jnp.dot(tok[blk, cols], wg[cols], preferred_element_type=F32)
            coef[blk] += jnp.dot(tok[blk, cols], wu[cols], preferred_element_type=F32)

        @pl.loop(0, T // EB)
        def _(i):
            blk = rows(i * EB, EB)
            gate = act[blk]
            hT[:, blk] = (gate * jax.nn.sigmoid(gate) * coef[blk]).astype(BF16).T

    def slopes():
        @pl.loop(0, T // EB)
        def _(i):
            blk = rows(i * EB, EB)
            gate, up = act[blk], coef[blk]
            sig = jax.nn.sigmoid(gate)
            act[blk] = gate * sig
            coef[blk] = up * sig * (1.0 + gate * (1.0 - sig))

    def hidden_most():
        @pl.loop(0, T // MB)
        def _(i):
            blk, cols = rows(i * MB, MB), pl.ds(pl.multiple_of(most_at, Dn), most)
            dh[blk] = contract_last(cot[blk, cols], wd[:, cols])

    def hidden_last():
        @pl.loop(0, T // MB)
        def _(i):
            blk, cols = rows(i * MB, MB), rows(last_at, Dn)
            dh[blk] += contract_last(cot[blk, cols], wd[:, cols])

        @pl.loop(0, T // EB)
        def _(i):
            blk = rows(i * EB, EB)
            slot, within = lax.div(i, R // EB), lax.rem(i, R // EB)
            by_core = rows((lax.rem(slot, 2) * tps + lax.div(slot, 2)) * R + within * EB, EB)
            dhid = dh[blk]
            a = (dhid * coef[blk]).astype(BF16)
            b = (dhid * act[blk]).astype(BF16)
            dg[by_core] = a
            du[by_core] = b
            gT[:, blk] = a.T
            uT[:, blk] = b.T

    sources = {DOWN: (hT, cot), GATE: (gT, tok), UP: (uT, tok)}

    def own_part(w, d):
        lhs, rhs = sources[w]
        own[...] = jnp.dot(lhs[...], rhs[:, rows(d * Dn, Dn)], preferred_element_type=F32)

    strip = H // cuts

    def strips(ref, w, k, q):
        return ref.at[w, k, pl.ds(q * strip, strip)]

    def grad_send(w, d, q, there, to):
        remote(strips(rs, w, d, q), strips(rs, w, there, q), rs_send.at[w],
               rs_recv.at[w, there, q], to).start()

    def grad_add(w, k, q):
        arrived(strips(rs, w, k, q), rs_recv.at[w, k, q])
        return own[pl.ds(q * strip, strip)] + rs[w, k, pl.ds(q * strip, strip)].astype(F32)

    def grad_edge(w, d):
        @pl.when(jnp.where(f == 0, d > 0, jnp.logical_and(f == n - 1, d < n - 1)))
        def _():
            own_part(w, d)
            rs[w, d] = own[...].astype(BF16)
            there = jnp.where(jnp.logical_and(f > 0, d == f - 1), n, d)
            to = (r, jnp.where(f == 0, 1, n - 2), t)
            for q in range(cuts):
                grad_send(w, d, q, there, to)

    def grad_edge_group(w, g):
        per = n // groups

        @pl.loop(0, per)
        def _(i):
            grad_edge(w, g * per + jnp.where(f == 0, per - 1 - i, i))

    def grad_edges(w, first, last):
        @pl.loop(first, last)
        def _(i):
            grad_edge(w, jnp.where(f == 0, n - 1 - i, i))

    def grad_through(w, dist, far):
        onward = jnp.where((2 * f < n) == (not far), 1, -1)
        d = f + dist * onward
        here = jnp.logical_and(d >= 0, d < n)

        @pl.when(jnp.logical_and(here, jnp.logical_and(f > 0, f < n - 1)))
        def _():
            own_part(w, d)
            there = jnp.where(jnp.logical_and(onward < 0, d == f - 1), n, d)
            for q in range(cuts):
                rs[w, d, pl.ds(q * strip, strip)] = grad_add(w, d, q).astype(BF16)
                grad_send(w, d, q, there, (r, f + onward, t))

    def grad_through_far(w):
        if n > 3:
            @pl.loop(0, n - 3)
            def _(i):
                for far in (False, True):
                    grad_through(w, n - 2 - i, far)

    def grad_through_near(w, far):
        if n > 2:
            grad_through(w, 1, far)

    def grads_sent(w):
        all_sent(rs.at[w, pl.ds(0, n - 1)], rs_send.at[w])
        all_sent(xs.at[w], x_send.at[w])

    def grad_final(w):
        own_part(w, f)
        for q in range(cuts):
            @pl.when(f > 0)
            def _():
                own[pl.ds(q * strip, strip)] = grad_add(w, f, q)

            @pl.when(f < n - 1)
            def _():
                own[pl.ds(q * strip, strip)] = grad_add(w, n, q)

            xs[w, pl.ds(q * strip, strip)] = own[pl.ds(q * strip, strip)].astype(BF16)
            send(xs.at[w, pl.ds(q * strip, strip)], xr.at[w, pl.ds(q * strip, strip)],
                 x_send.at[w], x_recv.at[w], x_dev)

    def halves_arrived(w):
        arrived(xr.at[w], x_recv.at[w])

    KB = min(512, D)
    at_of = lambda rr, yy: rr * ny + yy

    def product(core, first, count, put):
        blk = pl.ds(pl.multiple_of((core * 2 * ny + first) * R, R), count * R)

        @pl.loop(0, D // KB)
        def _(k):
            cols = rows(k * KB, KB)
            put(cols, contract_last(dg[blk], wg[cols]) + contract_last(du[blk], wu[cols]))

    def block(ref, rr, dy):
        return ref.at[rows(at_of(rr, yat(dy)) * R, R)]

    def tokens_for_core(rr):
        blk = rows(rr * ny * R, ny * R)

        def put(cols, value):
            pc_s[blk, cols] = value.astype(BF16)
        product(1 - c, rr * ny, ny, put)
        for dy in list(others) + [0]:
            i = at_of(rr, yat(dy))
            send(block(pc_s, rr, dy), block(pc_r, rr, dy), pc_ss, pc_rs.at[i], core_dev)

    def tokens_own(rr, dys):
        for dy in dys:
            arrived(block(pc_r, rr, dy), pc_rs.at[at_of(rr, yat(dy))])
        groups_of = [(rr * ny, ny)] if len(dys) == ny else [(at_of(rr, yat(dy)), 1) for dy in dys]
        for first, count in groups_of:
            blk = pl.ds(pl.multiple_of(first * R, R), count * R)

            def put(cols, value):
                pc_r[blk, cols] = (value + pc_r[blk, cols].astype(F32)).astype(BF16)
            product(c, first, count, put)

    quarter = R // 4
    spans = [(k * quarter, quarter) for k in range(4)]
    EC = R // 8

    def span_at(ref, span):
        return ref.at[pl.ds(span[0], span[1])]

    def add_span(rr, dy, span, refs):
        start = at_of(rr, yat(dy)) * R + span[0]

        @pl.loop(0, span[1] // EC)
        def _(k):
            here = rows(start + k * EC, EC)
            total = pc_r[here].astype(F32)
            for ref in refs:
                total += ref[rows(span[0] + k * EC, EC)].astype(F32)
            pc_r[here] = total.astype(BF16)

    def to_y(rr, which, dy, span, k):
        send(span_at(block(pc_r, rr, dy), span), span_at(py_r.at[which, dy - 1], span),
             py_ss.at[which], py_rs.at[which, dy - 1, k], y_dev(dy))

    def from_y(which, dy, span, k):
        arrived(span_at(py_r.at[which, dy - 1], span), py_rs.at[which, dy - 1, k])

    def to_x(k):
        send(span_at(block(pc_r, 1 - r, 0), spans[k]), span_at(px_r, spans[k]), px_ss, px_rs.at[k], x_dev)

    def y_out(rr, which):
        for k, span in enumerate(spans):
            for dy in others:
                to_y(rr, which, dy, span, k)

    def x_piece(k):
        for dy in others:
            from_y(0, dy, spans[k], k)
        add_span(1 - r, 0, spans[k], [py_r.at[0, dy - 1] for dy in others])
        to_x(k)

    def tokens_final():
        for k, span in enumerate(spans):
            arrived(span_at(px_r, span), px_rs.at[k])
            for dy in others:
                from_y(1, dy, span, k)
        add_span(r, 0, (0, R), [px_r] + [py_r.at[1, dy - 1] for dy in others])
        put_out(block(pc_r, r, 0), gt_out, 0)

    def squares(value):
        return jnp.sum(value * value, axis=0, keepdims=True)

    outs = []

    def put_out(src, dst, k):
        copy = pltpu.make_async_copy(src, dst, out_sem.at[k])
        copy.start()
        outs.append(copy)

    def turn(w, k, buf, at, out):
        turned[w - 1, k] = buf[w].astype(F32).T.astype(BF16)
        dst = out.at[:, rows(at * H, H)] if sliced else out.at[at]
        put_out(turned.at[w - 1, k], dst, 2 * w + k + 1)

    def wide_mine(w, out):
        tnorm[mine, pl.ds(w - 1, 1)] = squares(xs[w].astype(F32))
        turn(w, 0, xs, r, out)

    def wide_theirs(w, out):
        halves_arrived(w)
        turn(w, 1, xr, 1 - r, out)

    def wide_norms_out():
        for i in range(2):
            for k in range(tps):
                if i or k:
                    to = (r if i == 0 else 1 - r, f, lax.rem(t + k, tps))
                    send(tnorm.at[mine], tnorm.at[mine], tn_ss, tn_rs, to)

    def wide_norms_in():
        arrived(tnorm.at[pl.ds(0, 2 * tps - 1)], tn_rs)
        t_sum[...] = jnp.sum(tnorm[...], axis=0)
        put_out(t_sum, tn_out, 7)

    def finish_down():
        for k, (buf, at) in enumerate(((xs, r), (xr, 1 - r))):
            if k:
                halves_arrived(DOWN)
            put_out(buf.at[DOWN], gd_out.at[at], k + 1)
            fnorm[f, pl.ds(at, 1)] = squares(buf[DOWN].astype(F32).T)

    def norms_out():
        for i in range(1, n):
            send(fnorm.at[f], fnorm.at[f], fn_ss, fn_rs, (r, lax.rem(f + i, n), t))

    def norms_in():
        arrived(fnorm.at[pl.ds(0, n - 1)], fn_rs)
        f_sum[...] = jnp.sum(fnorm[...], axis=0)
        put_out(f_sum, fn_out, 8)

    order = [jnp.where(2 * f < n, groups - 1 - g, g) for g in range(groups)]

    for load in loads[:3]:
        load.wait()
    tok_out(1, 0)
    weights_step(GATE, 0)
    weights_step(UP, 0)
    tok_out(0, 1)
    for h in (0, 1):
        send_piece(*tok_piece(mine, h), core_dev)
    for load in loads[3:]:
        load.wait()
    for g in order:
        cot_send(mine, g, None, core_dev)
    tnorm[mine] = jnp.zeros(tnorm.shape[1:], F32)
    fnorm[f] = jnp.zeros(fnorm.shape[1:], F32)
    if n > 2:
        weights_step(GATE, 1)
    tok_first()
    cot_out(order[0])
    tok_first_core()
    if n > 2:
        weights_step(UP, 1)
    tok_second()
    if groups > 1:
        cot_out(order[1])
    for s in range(2, n - 1):
        weights_step(GATE, s)
        weights_step(UP, s)
    weights_step(DOWN, 0)
    tok_diagonal()
    tok_from_core()
    steps = T // MB
    gate_up_most(0, steps // 2)

    def cot_next(k):
        cot_first(order[k])
        if k + 2 < groups:
            cot_out(order[k + 2])
        cot_first_core(order[k])

    cot_next(0)
    gate_up_most(steps // 2, steps)
    if groups > 1:
        cot_next(1)
    weights_step(GATE, n - 1)
    weights_step(UP, n - 1)
    cot_diagonal(order[0])
    gate_up_last()
    if groups > 2:
        cot_next(2)
    cot_from_core(order[0])
    grad_edge_group(DOWN, order[0])
    slopes()
    down_steps = list(range(1, n - 1))
    for s in down_steps[:1]:
        weights_step(DOWN, s)
    for k in range(1, groups):
        cot_diagonal(order[k])
        if k + 2 < groups:
            cot_next(k + 2)
        cot_from_core(order[k])
        grad_edge_group(DOWN, order[k])
        if n == 4 and k == groups - 2:
            grad_through_far(DOWN)
        for s in down_steps[k:k + 1]:
            weights_step(DOWN, s)
    for s in down_steps[groups:]:
        weights_step(DOWN, s)
    if n != 4:
        grad_through_far(DOWN)
    hidden_most()
    weights_step(DOWN, n - 1)
    hidden_last()
    grad_edges(GATE, 0, 1)
    grad_through_near(DOWN, False)
    grad_through_near(DOWN, True)
    tokens_for_core(1 - r)
    grad_edges(GATE, 1, n - 1)
    tokens_for_core(r)
    tokens_own(1 - r, list(others))
    y_out(1 - r, 0)
    grad_final(DOWN)
    grad_through_far(GATE)
    tokens_own(1 - r, [0])
    tokens_own(r, list(range(ny)))
    y_out(r, 1)
    grad_edges(UP, 0, n - 1)
    grad_through_near(GATE, True)
    grad_through_near(GATE, False)
    x_piece(0)
    finish_down()
    norms_out()
    x_piece(1)
    x_piece(2)
    grad_final(GATE)
    x_piece(3)
    wide_mine(GATE, gg_out)
    grad_through_far(UP)
    grad_through_near(UP, True)
    grad_through_near(UP, False)
    grad_final(UP)
    wide_mine(UP, gu_out)
    wide_norms_out()
    wide_theirs(GATE, gg_out)
    tokens_final()
    wide_theirs(UP, gu_out)
    norms_in()
    wide_norms_in()

    for copy in outs:
        copy.wait()
    for a, buf in enumerate((tok, cot)):
        all_sent(buf.at[pl.ds(0, sent[a] // D)], ag_send.at[a])
    for w in (DOWN, GATE, UP):
        weights_sent(w)
        grads_sent(w)
    all_sent(pc_s, pc_ss)
    if ny > 1:
        for which in (0, 1):
            all_sent(py_r.at[which], py_ss.at[which])
    all_sent(px_r, px_ss)
    all_sent(tnorm.at[pl.ds(0, 2 * tps - 1)], tn_ss)
    all_sent(fnorm.at[pl.ds(0, n - 1)], fn_ss)


def widen(gt, gg, gu, gd, tn, fn, gt_out, gg_out, gu_out, gd_out, g_norm, u_norm, d_norm):
    gt_out[...] = gt[...]
    for src, dst in ((gg, gg_out), (gu, gu_out), (gd, gd_out)):
        dst[...] = src[...].astype(F32)
    g_norm[...] = tn[0:1]
    u_norm[...] = tn[1:2]
    if len(d_norm.shape) == 1:
        size = fn.shape[1]
        d_norm[0:size] = fn[0]
        d_norm[size:] = fn[1]
    else:
        d_norm[...] = fn[0:2]


def local(tokens, cotangent, gate_weight, up_weight, down_weight):
    n, tps = lax.axis_size("fs"), lax.axis_size("tp")
    ny = tps // 2
    R, D = tokens.shape
    H = gate_weight.shape[1] // 2
    T, Dn = 2 * tps * R, D // n
    sliced = H % 128 == 0
    if not sliced:
        r = lax.axis_index("rep")
        gate_weight = lax.dynamic_slice_in_dim(gate_weight, r * H, H, 1)
        up_weight = lax.dynamic_slice_in_dim(up_weight, r * H, H, 1)
        down_weight = lax.dynamic_slice_in_dim(down_weight, r * H, H, 0)
    blocks = 2 * tps
    groups, cuts = min(n, 4), 4
    wide_shape = (Dn, 2 * H) if sliced else (2, Dn, H)
    more = max(ny - 1, 1)
    vmem = pltpu.VMEM
    one = pltpu.SemaphoreType.DMA
    dma = lambda *shape: one(shape)
    shape = jax.ShapeDtypeStruct
    any_spec = pl.BlockSpec(memory_space=pl.ANY)
    flops = 2 * 8 * T * D * H
    gt, gg, gu, gd, tn, fn = pl.pallas_call(
        functools.partial(kernel, n, tps, sliced, groups, cuts),
        out_shape=(
            shape((R, D), BF16), shape(wide_shape, BF16), shape(wide_shape, BF16),
            shape((2, H, Dn), BF16), shape((8, Dn), F32), shape((8, H), F32)),
        in_specs=[any_spec] * 5,
        out_specs=(any_spec,) * 6,
        scratch_shapes=[
            vmem((T, D), BF16), vmem((T, D), BF16),
            vmem((D, H), BF16), vmem((D, H), BF16), vmem((H, D), BF16),
            vmem((T, H), F32), vmem((T, H), F32), vmem((T, H), F32),
            vmem((H, T), BF16), vmem((H, T), BF16), vmem((H, T), BF16),
            vmem((T, H), BF16), vmem((T, H), BF16), vmem((H, Dn), F32),
            vmem((3, n + 1, H, Dn), BF16), vmem((3, H, Dn), BF16), vmem((3, H, Dn), BF16),
            vmem((2 * ny * R, D), BF16), vmem((2 * ny * R, D), BF16),
            vmem((2, more, R, D), BF16), vmem((R, D), BF16),
            vmem((2, 2, Dn, H), BF16), vmem((blocks, 8, Dn), F32), vmem((n, 8, H), F32), vmem((8, Dn), F32), vmem((8, H), F32),
            dma(5), dma(2), dma(blocks, 2), dma(blocks, groups),
            dma(3, 2, n - 1), dma(3, n), dma(3), dma(3, n + 1, cuts), dma(3), dma(3),
            one, dma(2 * ny), dma(2), dma(2, more, 4), one, dma(4),
            one, one, one, one, dma(9),
        ],
        compiler_params=pltpu.CompilerParams(
            collective_id=0, has_side_effects=True, vmem_limit_bytes=67043328),
        cost_estimate=pl.CostEstimate(flops=flops, bytes_accessed=16 << 20, transcendentals=T * H),
    )(tokens, cotangent, gate_weight, up_weight, down_weight)
    if not sliced:
        gg, gu = (jnp.concatenate([part[0], part[1]], axis=1) for part in (gg, gu))
    steps = 2
    pieces = [(R, D), (Dn, 2 * H), (Dn, 2 * H), (2 * H, Dn)]
    tiles = [pl.BlockSpec((rows // steps, cols), lambda i: (i, 0)) for rows, cols in pieces]
    whole = lambda *dims: pl.BlockSpec(dims, lambda i: (0,) * len(dims))
    norms = [(1, Dn), (1, Dn), (2 * H,) if sliced else (2, H)]
    outs = pl.pallas_call(
        widen,
        grid=(steps,),
        out_shape=[shape(piece, F32 if i else BF16) for i, piece in enumerate(pieces)]
        + [shape(norm, F32) for norm in norms],
        in_specs=tiles + [whole(8, Dn), whole(8, H)],
        out_specs=tiles + [whole(*norm) for norm in norms],
    )(gt, gg, gu, gd.reshape(2 * H, Dn), tn, fn)
    return tuple(outs[:4]) + tuple(out.reshape(-1) for out in outs[4:])


def solution(mesh):
    placed = (
        P(("rep", "fs", "tp"), None),
        P(("rep", "fs", "tp"), None),
        P("fs", "tp"),
        P("fs", "tp"),
        P("tp", "fs"),
    )
    return jax.shard_map(
        local,
        mesh=mesh,
        in_specs=placed,
        out_specs=(
            P(("rep", "fs", "tp"), None),
            P("fs", "tp"),
            P("fs", "tp"),
            P("tp", "fs"),
            P("fs"),
            P("fs"),
            P("tp"),
        ),
        check_vma=False,
    )
```
